128 devices in a mesh: sp: 32 (over z, y, core), tp: 4 (over x).
Axes of the slice: x: 4, y: 4, z: 4, core: 2. Of those that a mesh axis runs over, the one named last changes fastest.
Arguments:
- queries: bfloat16 [16384, 2048], P('sp', 'tp'), may hold values from -6 to 6
- keys: bfloat16 [16384, 512], P('sp', 'tp'), may hold values from -6 to 6
- values: bfloat16 [16384, 512], P('sp', 'tp'), may hold values from -6 to 6
- residual: bfloat16 [16384, 2048], P(('sp', 'tp')), may hold values from -0.119628906 to 0.119628906
- out_proj: bfloat16 [2048, 2048], replicated, may hold values from -0.125 to 0.125
- query_gain: float32 [128], replicated, may hold values from 0.7 to 7
- key_gain: float32 [128], replicated, may hold values from 0.7 to 7
- norm_gain: float32 [2048], replicated, may hold values from 0.1 to 1.9
- routes: int32 [16384, 4], P(('sp', 'tp')), may hold values from 0 to 127, all different within a row; in each aligned block of 128 rows (0 to 127, 128 to 255, ...) at most 8 rows name the same one
- route_weight: float32 [16384, 4], P(('sp', 'tp')), may hold values from 0.1 to 1
- expert_gate: bfloat16 [128, 2048, 256], P(('sp', 'tp')), may hold values from -0.125 to 0.125
- expert_up: bfloat16 [128, 2048, 256], P(('sp', 'tp')), may hold values from -0.125 to 0.125
- expert_down: bfloat16 [128, 256, 2048], P(('sp', 'tp')), may hold values from -0.375 to 0.375
- shared_gate: bfloat16 [2048, 256], replicated, may hold values from -0.125 to 0.125
- shared_up: bfloat16 [2048, 256], replicated, may hold values from -0.125 to 0.125
- shared_down: bfloat16 [256, 2048], replicated, may hold values from -0.375 to 0.375
Outputs:
- layer_out: bfloat16 [16384, 2048], P(('sp', 'tp'))
The draws below stay inside these ranges and needn't reach their ends.
Inputs may be any that keep to these rules, and one draw needn't show every extreme that they name: In the rows of one device (aligned blocks of 128 tokens), no expert is named by more than 8 routes; some expert is named by exactly 8 routes of some device; the 4 experts of a token differ.
All inputs are finite; a program needn't handle non-finite values.
Results may differ from the reference program's by a relative error of at most 0.023.
The reference program's roundings to bfloat16 on the way count: a program that leaves them out, or rounds other values in their place, can miss the bound.
Values may be sent and summed in bfloat16 or wider, within the bound.
No kernel may reach another device: no remote copies, remote signals or barrier semaphores. Data moves between devices by JAX's collectives and lax.ppermute only.
A program may use at most 128 MiB of HBM per device.

```python
import math
import jax
import jax.numpy as jnp
import numpy as np
from jax import lax

D = 2048
HEADS = 16
KV_HEADS = 4
HD = 128
EFF = 256
SFF = 256
GRID_W = 64
TOP = 4
SEQ = 16384
ROWS_DEV = 128
EXPERTS = 128
CAP = 8
N_SP = 32
N_TP = 4


def paired_draw(key):
    key_rows = jax.random.normal(jax.random.fold_in(key, 11), (SEQ, KV_HEADS * HD), jnp.float32)
    query_rows = jax.random.normal(jax.random.fold_in(key, 12), (SEQ, HEADS * HD), jnp.float32)
    return (jnp.clip(query_rows, -6.0, 6.0), jnp.clip(key_rows, -6.0, 6.0))


def draw_queries(key, part):
    return paired_draw(key)[0].astype(jnp.bfloat16)


def draw_keys(key, part):
    return paired_draw(key)[1].astype(jnp.bfloat16)


def gain_draw(key):
    return jax.random.uniform(key, (HD,), jnp.float32, 0.7, 1.3)


def draw_query_gain(key, part):
    return gain_draw(jax.random.fold_in(key, 21))


def draw_key_gain(key, part):
    return gain_draw(jax.random.fold_in(key, 22))


def block_scale(rng, shape, cuts, low, largest):
    def one(dim, blocks):
        heights = jax.random.uniform(jax.random.fold_in(jax.random.fold_in(rng, 6), dim), (blocks,), jnp.float32, low / len(cuts), largest / len(cuts))
        return jnp.repeat(jnp.exp(heights), shape[dim] // blocks).reshape((-1,) + (1,) * (len(shape) - dim - 1))

    loudness = one(*cuts[0])
    for cut in cuts[1:]:
        loudness = loudness * one(*cut)
    return loudness


def deal_out(own_key, own, number, rows, amount, top, limit, slope):
    ranking = jax.random.permutation(own_key, amount)
    heavy_load, common = portions_of(amount, rows * top, limit, slope, True), portions_of(amount, rows * top, limit, slope, False)
    places = jnp.arange(amount)

    def named(sizes, rotation):
        used = int((sizes > 0).sum())
        fixed = max(1, used // 4)
        passed = fixed + (places - fixed + rotation * (used - fixed)) % max(1, amount - fixed)
        return jnp.zeros((amount,), jnp.int32).at[ranking[jnp.where(places < fixed, places, passed)]].set(jnp.asarray(sizes, jnp.int32))

    sizes = jnp.where(number % 4 == 0, named(heavy_load, number // 4), named(common, number - number // 4 - 1))
    mixed = jax.random.permutation(jax.random.fold_in(own, 3), amount)
    source_of, taker = mixed[0:amount // 2 * 2:2], mixed[1:amount // 2 * 2:2]
    margin = jnp.minimum(sizes[source_of] - 1, limit - sizes[taker]) // 2
    margin = jnp.where((source_of == ranking[0]) | (taker == ranking[0]) | (sizes[taker] == 0), 0, jnp.maximum(margin, 0))
    passed = jax.random.randint(jax.random.fold_in(own, 4), (amount // 2,), 0, 1 << 20) % (margin + 1)
    sizes = sizes.at[source_of].add(-passed).at[taker].add(passed)
    members = jnp.searchsorted(jnp.cumsum(sizes), jnp.arange(rows * top), side="right").astype(jnp.int32)
    listing = members.reshape(top, rows).T
    listing = listing[jax.random.permutation(jax.random.fold_in(own, 1), rows)]
    rotation = jax.random.randint(jax.random.fold_in(own, 2), (rows, 1), 0, top)
    return jnp.take_along_axis(listing, (jnp.arange(top)[None, :] + rotation) % top, axis=1)


def portions_of(count, total, limit, lean, full):
    portions = [(1 << 20) // math.isqrt(standing ** lean) + 1 for standing in range(1, count + 1)]
    largest = limit if full else min(limit, max(-(-total // count), total * portions[0] // sum(portions)))
    least = 1 if total - largest >= count - 1 else 0
    given, rest = [largest] + [least] * (count - 1), total - largest - least * (count - 1)
    while rest > 0:
        movable = [i for i in range(1, count) if given[i] < largest] or [i for i in range(1, count) if given[i] < limit]
        pool, remaining = sum([portions[i] for i in movable]), rest
        for i in movable:
            extra = min(limit - given[i], max(1, remaining * portions[i] // pool), rest)
            given[i] = given[i] + extra
            rest = rest - extra
    return np.array(given)


def gaussian(key, shape, spread, reach, cuts=(), kind=jnp.bfloat16):
    loudness = block_scale(key, shape, cuts, -0.22, 0.18) if cuts else 1.0
    values = jax.random.normal(key, shape, jnp.float32) * spread * loudness
    return jnp.minimum(jnp.maximum(values, -reach), reach).astype(kind)


def setup_inputs(seed: int = 0) -> dict:
    key_of = jax.random.split(jax.random.key(seed), 17)
    queries = draw_queries(jax.random.fold_in(key_of[16], 71), 0)
    keys = draw_keys(jax.random.fold_in(key_of[16], 71), 0)
    values = gaussian(key_of[2], (SEQ, KV_HEADS * HD), 1.0, 6.0, ((0, 32), (1, 4)))
    residual = gaussian(key_of[3], (SEQ, D), 0.02, 0.119628906, ((0, 128),))
    out_proj = gaussian(key_of[4], (HEADS * HD, D), (HEADS * HD) ** -0.5, 0.125)
    query_gain = draw_query_gain(jax.random.fold_in(key_of[16], 71), 0)
    key_gain = draw_key_gain(jax.random.fold_in(key_of[16], 71), 0)
    norm_gain = jnp.clip(1.0 + 0.18 * jax.random.normal(key_of[7], (D,), jnp.float32), 0.1, 1.9)
    routes_keys = jax.random.split(jax.random.fold_in(key_of[8], 1), SEQ // ROWS_DEV)
    routes_turns = jax.random.permutation(jax.random.fold_in(key_of[8], 3), SEQ // ROWS_DEV)
    routes = jax.vmap(lambda own, number: deal_out(jax.random.fold_in(key_of[8], 2), own, number, ROWS_DEV, EXPERTS, TOP, CAP, 2))(routes_keys, routes_turns).reshape((SEQ, TOP))
    route_weight = jnp.clip(jnp.exp(math.log(1.0) - 2.3025851 * jax.random.uniform(key_of[9], (SEQ, TOP), jnp.float32) ** block_scale(key_of[9], (SEQ, TOP), ((0, 128),), -0.2, 0.2)), 0.1, 1.0)
    expert_gate = gaussian(key_of[10], (EXPERTS, D, EFF), D ** -0.5, 0.125, ((0, 128),))
    expert_up = gaussian(key_of[11], (EXPERTS, D, EFF), D ** -0.5, 0.125, ((0, 128),))
    expert_down = gaussian(key_of[12], (EXPERTS, EFF, D), EFF ** -0.5, 0.375, ((0, 128),))
    shared_gate = gaussian(key_of[13], (D, SFF), D ** -0.5, 0.125)
    shared_up = gaussian(key_of[14], (D, SFF), D ** -0.5, 0.125)
    shared_down = gaussian(key_of[15], (SFF, D), SFF ** -0.5, 0.375)
    return dict(queries=queries, keys=keys, values=values, residual=residual, out_proj=out_proj, query_gain=query_gain, key_gain=key_gain, norm_gain=norm_gain, routes=routes, route_weight=route_weight, expert_gate=expert_gate, expert_up=expert_up, expert_down=expert_down, shared_gate=shared_gate, shared_up=shared_up, shared_down=shared_down)


EPS = 1e-06
THETA = 10000.0

def rotate_pairs(block, cosine, sine):
    first, second = jnp.split(block, 2, axis=-1)
    return jnp.concatenate([first * cosine - second * sine, second * cosine + first * sine], axis=-1)

def normed_rotary(source, gain, heads, offset):
    count = source.shape[0]
    width = gain.shape[0]
    values_f = source.astype(jnp.float32).reshape(count, heads, width)
    values_f = values_f * lax.rsqrt(lax.optimization_barrier(jnp.mean(values_f * values_f, axis=-1, keepdims=True)) + EPS) * gain
    position = offset + jnp.arange(count, dtype=jnp.int32)
    grid_row = (position // GRID_W).astype(jnp.float32)
    grid_col = (position % GRID_W).astype(jnp.float32)
    quarter = width // 4
    inverse = jnp.power(THETA, -4.0 * jnp.arange(quarter, dtype=jnp.float32) / width)
    row_angle = (grid_row[:, None] * inverse[None, :])[:, None, :]
    col_angle = (grid_col[:, None] * inverse[None, :])[:, None, :]
    row_half, col_half = jnp.split(values_f, 2, axis=-1)
    turned = jnp.concatenate([rotate_pairs(row_half, jnp.cos(row_angle), jnp.sin(row_angle)), rotate_pairs(col_half, jnp.cos(col_angle), jnp.sin(col_angle))], axis=-1)
    return turned.reshape(count, heads * width).astype(jnp.bfloat16)

def reference(queries, keys, values, residual, out_proj, query_gain, key_gain, norm_gain, routes, route_weight, expert_gate, expert_up, expert_down, shared_gate, shared_up, shared_down):
    tokens = queries.shape[0]
    width = query_gain.shape[0]
    group = HEADS // KV_HEADS
    scale = 1.0 / math.sqrt(width)
    q_rot = normed_rotary(queries, query_gain, HEADS, 0)
    k_rot = normed_rotary(keys, key_gain, KV_HEADS, 0)
    key_f = k_rot.reshape(tokens, KV_HEADS, width).astype(jnp.float32).transpose(1, 0, 2)
    value_f = values.reshape(tokens, KV_HEADS, width).astype(jnp.float32).transpose(1, 0, 2)
    block = math.gcd(tokens, 512)
    q_blocks = q_rot.reshape(tokens // block, block, KV_HEADS, group, width).transpose(0, 2, 3, 1, 4)

    def attend_head(operands):
        query_part, key_part, value_part = operands
        scores = jnp.einsum('gqd,kd->gqk', query_part.astype(jnp.float32), key_part) * scale
        top = lax.optimization_barrier(jnp.max(scores, axis=-1, keepdims=True))
        weights = jnp.exp(scores - top)
        denom = lax.optimization_barrier(jnp.sum(weights, axis=-1, keepdims=True))
        rounded = weights.astype(jnp.bfloat16).astype(jnp.float32)
        summed = jnp.einsum('gqk,kd->gqd', rounded, value_part)
        return (summed / denom).astype(jnp.bfloat16)

    def attend_block(query_block):
        return lax.map(attend_head, (query_block, key_f, value_f))
    outputs = lax.map(attend_block, q_blocks)
    attn_heads = outputs.transpose(0, 3, 1, 2, 4).reshape(tokens, HEADS * width)
    projected = jnp.dot(attn_heads, out_proj, preferred_element_type=jnp.float32)
    hidden1 = (residual.astype(jnp.float32) + projected).astype(jnp.bfloat16)
    hidden_f = hidden1.astype(jnp.float32)
    normed = (hidden_f * lax.rsqrt(lax.optimization_barrier(jnp.mean(hidden_f * hidden_f, axis=-1, keepdims=True)) + EPS) * norm_gain).astype(jnp.bfloat16)
    shared_hidden = (jax.nn.silu(jnp.dot(normed, shared_gate, preferred_element_type=jnp.float32)) * jnp.dot(normed, shared_up, preferred_element_type=jnp.float32)).astype(jnp.bfloat16)
    shared_out = jnp.dot(shared_hidden, shared_down, preferred_element_type=jnp.float32)
    pairs = tokens * TOP
    flat_routes = routes.reshape(pairs)
    bound = N_SP * N_TP * CAP
    padded = jnp.concatenate([normed, jnp.zeros((1, normed.shape[1]), jnp.bfloat16)], axis=0)

    def one_expert(expert, buffer):
        picked = jnp.nonzero(flat_routes == expert, size=bound, fill_value=pairs)[0].astype(jnp.int32)
        rows = padded[picked // TOP]
        hidden_e = (jax.nn.silu(jnp.dot(rows, expert_gate[expert], preferred_element_type=jnp.float32)) * jnp.dot(rows, expert_up[expert], preferred_element_type=jnp.float32)).astype(jnp.bfloat16)
        result = jnp.dot(hidden_e, expert_down[expert], preferred_element_type=jnp.float32).astype(jnp.bfloat16)
        return buffer.at[picked].set(result)
    buffer = lax.fori_loop(0, EXPERTS, one_expert, jnp.zeros((pairs + 1, normed.shape[1]), jnp.bfloat16))
    routed = buffer[:pairs].reshape(tokens, TOP, normed.shape[1]).astype(jnp.float32)
    mixed = jnp.einsum('tk,tkd->td', route_weight, routed) + shared_out
    return (hidden_f + mixed).astype(jnp.bfloat16)
```

```python
import functools
import math

import jax
import jax.numpy as jnp
import numpy as np
from jax import lax
from jax.experimental import pallas as pl
from jax.experimental.pallas import tpu as pltpu
from jax.sharding import Mesh
from jax.sharding import PartitionSpec as P

HEADS = 16
KV_HEADS = 4
GRID_W = 64
HD = 128
CAP = 8
EPS = 1e-06
THETA = 10000.0
LOG2E = math.log2(math.e)
SAFE = 80.0
CHUNKS = 4
VM = pltpu.VMEM


def vspec():
    return pl.BlockSpec(memory_space=VM)


def rotary_tables():
    quarter = HD // 4
    inverse = np.power(THETA, -4.0 * np.arange(quarter, dtype=np.float64) / HD).astype(np.float32)
    angles = (np.arange(256, dtype=np.float32)[:, None] * inverse[None, :]).astype(np.float64)
    cos, sin = np.cos(angles), np.sin(angles)
    cosine = np.concatenate([cos, cos, cos, cos], axis=1).astype(np.float32)
    sine = np.concatenate([-sin, sin, -sin, sin], axis=1).astype(np.float32)
    return cosine, sine


def turned(x, gain, cosine, sine):
    x = x * lax.rsqrt(jnp.mean(x * x, axis=-1, keepdims=True) + EPS) * gain
    lane = lax.broadcasted_iota(jnp.int32, x.shape, 1)
    partner = jnp.where((lane // 32) % 2 == 0, pltpu.roll(x, 96, 1), pltpu.roll(x, 32, 1))
    return x * cosine + partner * sine


def table_pair(row_cos, row_sin, col_cos, col_sin, row):
    lane = lax.broadcasted_iota(jnp.int32, (GRID_W, HD), 1)
    cosine = jnp.where(lane < 64, row_cos[pl.ds(row, 1), :], col_cos[0:GRID_W, :])
    sine = jnp.where(lane < 64, row_sin[pl.ds(row, 1), :], col_sin[0:GRID_W, :])
    return cosine, sine


def kv_prep_kernel(key_ref, value_ref, gain_ref, cos_ref, sin_ref, *out_refs):
    tokens = key_ref.shape[0]
    first_row = lax.axis_index("sp") * (tokens // GRID_W)
    gain = gain_ref[...]
    for c, out_ref in enumerate(out_refs):
        for half in range(2):
            block = 2 * c + half
            cosine, sine = table_pair(cos_ref, sin_ref, cos_ref, sin_ref, first_row + block)
            x = key_ref[GRID_W * block : GRID_W * (block + 1), :].astype(jnp.float32)
            out_ref[GRID_W * half : GRID_W * (half + 1), :] = turned(x, gain, cosine, sine).astype(
                jnp.bfloat16
            )
        v = value_ref[HD * c : HD * (c + 1), :].astype(jnp.float32)
        out_ref[HD : 2 * HD, :] = v.T.astype(jnp.bfloat16)


def q_prep_kernel(query_ref, gain_ref, cos_ref, sin_ref, out_ref):
    tokens = query_ref.shape[0]
    group = query_ref.shape[1] // HD
    first_row = lax.axis_index("sp") * (tokens // GRID_W)
    gain = gain_ref[...]
    factor = LOG2E / math.sqrt(HD)
    for pair in range(tokens // HD):
        tables = [
            table_pair(cos_ref, sin_ref, cos_ref, sin_ref, first_row + 2 * pair + half)
            for half in range(2)
        ]
        for head in range(group):
            parts = []
            for half in range(2):
                at = HD * pair + GRID_W * half
                x = query_ref[at : at + GRID_W, HD * head : HD * (head + 1)].astype(jnp.float32)
                r = turned(x, gain, *tables[half])
                parts.append(r.astype(jnp.bfloat16).astype(jnp.float32))
            flat = jnp.concatenate(parts, axis=0).T * factor
            high = flat.astype(jnp.bfloat16)
            low = (flat - high.astype(jnp.float32)).astype(jnp.bfloat16)
            column = head * tokens + HD * pair
            out_ref[0:HD, column : column + HD] = high
            out_ref[HD : 2 * HD, column : column + HD] = low


def attention_kernel(
    first, last, qt_ref, kv_ref, qg_ref, kg_ref, *rest
):
    if first:
        state_in = None
        outs = rest
    else:
        state_in = rest[:3]
        outs = rest[3:]
    rows = 64
    blocks = kv_ref.shape[0]
    tiles = blocks // 2
    columns = qt_ref.shape[1]
    if last:
        final_ref, acc_ref, sum_ref, max_ref = outs
    else:
        acc_ref, sum_ref, max_ref = outs
    bound = jnp.max(jnp.abs(qg_ref[...])) * jnp.max(jnp.abs(kg_ref[...]))
    bound = bound * (1.02 * LOG2E * math.sqrt(HD))
    safe = bound <= SAFE

    def scoped(*accs):
        scores = [[[accs[(b * 2 + m) * 4 + r] for r in range(4)] for m in range(2)] for b in range(3)]
        total = [accs[24 + m] for m in range(2)]

        def query_key(tile, slot, base):
            for m in range(2):
                pltpu.matmul_push_rhs(
                    qt_ref[:, pl.ds(base + 256 * m, 256)], staging_register=0, mxu_index=m
                )
            for r in range(4):
                k = kv_ref[2 * tile + r // 2, (r % 2) * rows : (r % 2 + 1) * rows, :]
                kk = jnp.concatenate([k, k], axis=1)
                for m in range(2):
                    pltpu.matmul_acc_lhs(
                        scores[slot][m][r], kk, load_staged_rhs=0 if r == 0 else None
                    )

        def weigh_values(tile, slot, sums, shifts):
            sums = list(sums)
            for m in range(2):
                pieces = []
                for r in range(4):
                    s = pltpu.matmul_pop(scores[slot][m][r])
                    if shifts is not None:
                        s = s - shifts[m]
                    e = jnp.exp2(s)
                    sums[m] = sums[m] + jnp.sum(e.reshape(rows // 8, 8, 256), axis=0)
                    pieces.append(e.astype(jnp.bfloat16))
                pltpu.matmul_push_rhs(
                    jnp.concatenate(pieces, axis=0), staging_register=1, mxu_index=m
                )
            v = jnp.concatenate(
                [kv_ref[2 * tile, HD : 2 * HD, :], kv_ref[2 * tile + 1, HD : 2 * HD, :]], axis=1
            )
            for m in range(2):
                pltpu.matmul_acc_lhs(total[m], v, load_staged_rhs=1)
            return tuple(sums)

        zero_sums = tuple(jnp.zeros((8, 256), jnp.float32) for _ in range(2))

        @pl.when(safe)
        def _():
            def trip(j, carry):
                base = pl.multiple_of(j * 512, 512)
                query_key(0, 0, base)
                query_key(1, 1, base)
                sums = zero_sums
                for t in range(tiles):
                    if t + 2 < tiles:
                        query_key(t + 2, (t + 2) % 3, base)
                    sums = weigh_values(t, t % 3, sums, None)
                for m in range(2):
                    at = pl.ds(base + 256 * m, 256)
                    added = pltpu.matmul_pop(total[m])
                    if state_in is None:
                        acc_ref[:, at] = added
                        sum_ref[:, at] = sums[m]
                        max_ref[:, at] = jnp.zeros((8, 256), jnp.float32)
                    else:
                        acc_ref[:, at] = state_in[0][:, at] + added
                        sum_ref[:, at] = state_in[1][:, at] + sums[m]
                        max_ref[:, at] = state_in[2][:, at]
                return carry

            lax.fori_loop(0, columns // 512, trip, 0)

        @pl.when(jnp.logical_not(safe))
        def _():
            def trip(j, carry):
                base = pl.multiple_of(j * 512, 512)
                spans = [pl.ds(base + 256 * m, 256) for m in range(2)]

                def largest(t, tops):
                    query_key(t, 0, base)
                    new = []
                    for m in range(2):
                        top = tops[m]
                        for r in range(4):
                            s = pltpu.matmul_pop(scores[0][m][r])
                            top = jnp.maximum(top, jnp.max(s.reshape(rows // 8, 8, 256), axis=0))
                        new.append(top)
                    return tuple(new)

                if state_in is None:
                    old = tuple(jnp.full((8, 256), -1e30, jnp.float32) for _ in range(2))
                else:
                    old = tuple(state_in[2][:, at] for at in spans)
                tops = lax.fori_loop(0, tiles, largest, old)
                tops = [
                    jnp.broadcast_to(jnp.max(top, axis=0, keepdims=True), (8, 256)) for top in tops
                ]
                shifts = [top[0:1, :] for top in tops]

                def weigh(t, sums):
                    query_key(t, 0, base)
                    return weigh_values(t, 0, sums, shifts)

                sums = lax.fori_loop(0, tiles, weigh, zero_sums)
                for m, at in enumerate(spans):
                    added = pltpu.matmul_pop(total[m])
                    max_ref[:, at] = tops[m]
                    if state_in is None:
                        acc_ref[:, at] = added
                        sum_ref[:, at] = sums[m]
                    else:
                        factor = jnp.exp2(old[m] - tops[m])
                        acc_ref[:, at] = state_in[0][:, at] * factor[0:1, :] + added
                        sum_ref[:, at] = state_in[1][:, at] * factor + sums[m]
                return carry

            lax.fori_loop(0, columns // 512, trip, 0)

    specs = [pltpu.ACC(m)((rows, 256), jnp.float32) for _ in range(3) for m in range(2) for _ in range(4)]
    specs += [pltpu.ACC(m)((HD, 256), jnp.float32) for m in range(2)]
    pl.run_scoped(scoped, *specs)

    if last:
        tokens = final_ref.shape[0]

        def finish(i, carry):
            for head in range(columns // tokens):
                at = pl.ds(pl.multiple_of(head * tokens + i * HD, HD), HD)
                denom = jnp.sum(sum_ref[:, at], axis=0, keepdims=True)
                block = acc_ref[:, at] / denom
                final_ref[pl.ds(pl.multiple_of(i * HD, HD), HD), head * HD : (head + 1) * HD] = (
                    block.T.astype(jnp.bfloat16)
                )
            return carry

        lax.fori_loop(0, tokens // HD, finish, 0)


def attention_chunk(qt, kv, query_gain, key_gain, state, last, tokens):
    columns = qt.shape[1]
    first = state is None
    state_shapes = [
        jax.ShapeDtypeStruct((HD, columns), jnp.float32),
        jax.ShapeDtypeStruct((8, columns), jnp.float32),
        jax.ShapeDtypeStruct((8, columns), jnp.float32),
    ]
    keys = kv.shape[0] * HD
    flops = 4 * columns * keys * HD
    args = [qt, kv, query_gain, key_gain] + ([] if first else list(state))
    common = dict(
        in_specs=[vspec()] * len(args),
        compiler_params=pltpu.CompilerParams(vmem_limit_bytes=24 << 20),
        cost_estimate=pl.CostEstimate(flops=4 * flops, bytes_accessed=kv.size * 2, transcendentals=0),
        name="attention",
    )
    kernel = functools.partial(attention_kernel, first, last)
    if last:
        return pl.pallas_call(
            kernel,
            out_shape=jax.ShapeDtypeStruct((tokens, columns // tokens * HD), jnp.bfloat16),
            out_specs=vspec(),
            scratch_shapes=[VM(s.shape, s.dtype) for s in state_shapes],
            **common,
        )(*args)
    return pl.pallas_call(
        kernel, out_shape=state_shapes, out_specs=[vspec()] * 3, **common
    )(*args)


def route_kernel(routes_ref, weight_ref, place_ref, high_ref, low_ref):
    rows, top = routes_ref.shape
    experts = place_ref.shape[0] // CAP
    slots = place_ref.shape[0]
    routes = routes_ref[...]
    weight = weight_ref[...]
    expert = lax.broadcasted_iota(jnp.int32, (rows, experts), 1)
    chosen = jnp.zeros((rows, experts), jnp.float32)
    amount = jnp.zeros((rows, experts), jnp.float32)
    for k in range(top):
        hit = routes[:, k : k + 1] == expert
        chosen = jnp.where(hit, 1.0, chosen)
        amount = jnp.where(hit, weight[:, k : k + 1], amount)
    earlier = (
        lax.broadcasted_iota(jnp.int32, (rows, rows), 0)
        > lax.broadcasted_iota(jnp.int32, (rows, rows), 1)
    ).astype(jnp.bfloat16)
    rank = jnp.dot(earlier, chosen.astype(jnp.bfloat16), preferred_element_type=jnp.float32)
    wide = (
        lax.broadcasted_iota(jnp.int32, (experts, slots), 1) // CAP
        == lax.broadcasted_iota(jnp.int32, (experts, slots), 0)
    ).astype(jnp.bfloat16)
    slot = (lax.broadcasted_iota(jnp.int32, (rows, slots), 1) % CAP).astype(jnp.float32)

    def spread(x):
        return jnp.dot(x.astype(jnp.bfloat16), wide, preferred_element_type=jnp.float32)

    mine = (spread(rank) == slot) & (spread(chosen) > 0.5)
    place_ref[...] = mine.astype(jnp.float32).T.astype(jnp.bfloat16)
    high = amount.astype(jnp.bfloat16).astype(jnp.float32)
    high_ref[...] = jnp.where(mine, spread(high), 0.0).astype(jnp.bfloat16)
    low_ref[...] = jnp.where(mine, spread(amount - high), 0.0).astype(jnp.bfloat16)


def project_kernel(heads_ref, weight_ref, residual_ref, gain_ref, place_ref, hidden_ref, normed_ref, send_ref):
    parts = heads_ref.shape[0]
    depth = heads_ref.shape[2]
    total = residual_ref[...].astype(jnp.float32)
    heads = jnp.concatenate([heads_ref[i] for i in range(parts)], axis=1)
    total = total + jnp.dot(heads, weight_ref[...], preferred_element_type=jnp.float32)
    hidden = total.astype(jnp.bfloat16)
    hidden_ref[...] = hidden
    hidden = hidden.astype(jnp.float32)
    normed = (
        hidden
        * lax.rsqrt(jnp.mean(hidden * hidden, axis=-1, keepdims=True) + EPS)
        * gain_ref[...]
    ).astype(jnp.bfloat16)
    normed_ref[...] = normed
    send_ref[...] = jnp.dot(
        place_ref[...], normed, preferred_element_type=jnp.float32
    ).astype(jnp.bfloat16)


def combine_kernel(returned_ref, high_ref, low_ref, hidden_ref, normed_ref, sg_ref, su_ref, sd_ref, out_ref):
    normed = normed_ref[...]
    gate = jnp.dot(normed, sg_ref[...], preferred_element_type=jnp.float32)
    up = jnp.dot(normed, su_ref[...], preferred_element_type=jnp.float32)
    shared = (jax.nn.silu(gate) * up).astype(jnp.bfloat16)
    returned = returned_ref[...]
    total = jnp.dot(shared, sd_ref[...], preferred_element_type=jnp.float32)
    total = total + jnp.dot(high_ref[...], returned, preferred_element_type=jnp.float32)
    total = total + jnp.dot(low_ref[...], returned, preferred_element_type=jnp.float32)
    out_ref[...] = (hidden_ref[...].astype(jnp.float32) + total).astype(jnp.bfloat16)


def body(
    queries,
    keys,
    values,
    residual,
    out_proj,
    query_gain,
    key_gain,
    norm_gain,
    routes,
    route_weight,
    expert_gate,
    expert_up,
    expert_down,
    shared_gate,
    shared_up,
    shared_down,
):
    tokens = queries.shape[0]
    columns = queries.shape[1] // HD * tokens
    rows = residual.shape[0]
    model = residual.shape[1]
    experts = expert_gate.shape[0] * lax.axis_size("sp") * lax.axis_size("tp")
    slots = experts * CAP
    cosine, sine = (jnp.asarray(t) for t in rotary_tables())
    qg, kg = query_gain.reshape(1, HD), key_gain.reshape(1, HD)
    bf16 = jnp.bfloat16
    shape = jax.ShapeDtypeStruct
    pieces = pl.pallas_call(
        kv_prep_kernel,
        out_shape=[shape((2 * HD, HD), bf16)] * CHUNKS,
        in_specs=[vspec()] * 5,
        out_specs=[vspec()] * CHUNKS,
        name="kv_prep",
    )(keys, values, kg, cosine, sine)
    gathered = [lax.all_gather(p, "sp", axis=0, tiled=False) for p in pieces]
    qt = pl.pallas_call(
        q_prep_kernel,
        out_shape=shape((2 * HD, columns), bf16),
        in_specs=[vspec()] * 4,
        out_specs=vspec(),
        name="q_prep",
    )(queries, qg, cosine, sine)
    place, high, low = pl.pallas_call(
        route_kernel,
        out_shape=[shape((slots, rows), bf16), shape((rows, slots), bf16), shape((rows, slots), bf16)],
        in_specs=[vspec()] * 2,
        out_specs=[vspec()] * 3,
        name="route",
    )(routes, route_weight)
    state = None
    for c, kv in enumerate(gathered):
        state = attention_chunk(qt, kv, qg, kg, state, c == CHUNKS - 1, tokens)
    attn_local = state
    parts = tokens // rows
    all_heads = lax.all_to_all(
        attn_local.reshape(parts, rows, attn_local.shape[1]), "tp", split_axis=0, concat_axis=0, tiled=True
    )
    hidden1, normed, send = pl.pallas_call(
        project_kernel,
        out_shape=[shape((rows, model), bf16), shape((rows, model), bf16), shape((slots, model), bf16)],
        in_specs=[vspec()] * 5,
        out_specs=[vspec()] * 3,
        compiler_params=pltpu.CompilerParams(vmem_limit_bytes=40 << 20),
        name="project",
    )(all_heads, out_proj, residual, norm_gain.reshape(1, model), place)
    arrived = lax.all_to_all(
        send.reshape(experts, CAP, model), ("sp", "tp"), split_axis=0, concat_axis=0, tiled=True
    ).reshape(slots, model)
    gate = jnp.dot(arrived, expert_gate[0], preferred_element_type=jnp.float32)
    up = jnp.dot(arrived, expert_up[0], preferred_element_type=jnp.float32)
    hidden_e = (jax.nn.silu(gate) * up).astype(bf16)
    processed = jnp.dot(hidden_e, expert_down[0], preferred_element_type=jnp.float32).astype(bf16)
    returned = lax.all_to_all(
        processed.reshape(experts, CAP, model), ("sp", "tp"), split_axis=0, concat_axis=0, tiled=True
    ).reshape(slots, model)
    return pl.pallas_call(
        combine_kernel,
        out_shape=shape((rows, model), bf16),
        in_specs=[vspec()] * 8,
        out_specs=vspec(),
        compiler_params=pltpu.CompilerParams(vmem_limit_bytes=40 << 20),
        name="combine",
    )(returned, high, low, hidden1, normed, shared_gate, shared_up, shared_down)


def solution(mesh):
    placed = (
        P("sp", "tp"),
        P("sp", "tp"),
        P("sp", "tp"),
        P(("sp", "tp"), None),
        P(),
        P(),
        P(),
        P(),
        P(("sp", "tp"), None),
        P(("sp", "tp"), None),
        P(("sp", "tp"), None, None),
        P(("sp", "tp"), None, None),
        P(("sp", "tp"), None, None),
        P(),
        P(),
        P(),
    )
    return jax.shard_map(
        body, mesh=mesh, in_specs=placed, out_specs=P(("sp", "tp"), None), check_vma=False
    )
```

```python
import functools
import math

import jax
import jax.numpy as jnp
import numpy as np
from jax import lax
from jax.experimental import pallas as pl
from jax.experimental.pallas import tpu as pltpu
from jax.sharding import Mesh
from jax.sharding import PartitionSpec as P

HEADS = 16
KV_HEADS = 4
GRID_W = 64
HD = 128
CAP = 8
EPS = 1e-06
THETA = 10000.0
LOG2E = math.log2(math.e)
SAFE = 80.0
VM = pltpu.VMEM


def vspec():
    return pl.BlockSpec(memory_space=VM)


def rotary_tables():
    quarter = HD // 4
    inverse = np.power(THETA, -4.0 * np.arange(quarter, dtype=np.float64) / HD).astype(np.float32)
    angles = (np.arange(256, dtype=np.float32)[:, None] * inverse[None, :]).astype(np.float64)
    cos, sin = np.cos(angles), np.sin(angles)
    cosine = np.concatenate([cos, cos, cos, cos], axis=1).astype(np.float32)
    sine = np.concatenate([-sin, sin, -sin, sin], axis=1).astype(np.float32)
    return cosine, sine


def turned(x, gain, cosine, sine):
    x = x * lax.rsqrt(jnp.mean(x * x, axis=-1, keepdims=True) + EPS) * gain
    lane = lax.broadcasted_iota(jnp.int32, x.shape, 1)
    partner = jnp.where((lane // 32) % 2 == 0, pltpu.roll(x, 96, 1), pltpu.roll(x, 32, 1))
    return x * cosine + partner * sine


def table_pair(row_cos, row_sin, col_cos, col_sin, row):
    lane = lax.broadcasted_iota(jnp.int32, (GRID_W, HD), 1)
    cosine = jnp.where(lane < 64, row_cos[pl.ds(row, 1), :], col_cos[0:GRID_W, :])
    sine = jnp.where(lane < 64, row_sin[pl.ds(row, 1), :], col_sin[0:GRID_W, :])
    return cosine, sine


def kv_prep_kernel(key_ref, value_ref, gain_ref, cos_ref, sin_ref, out_ref):
    tokens = key_ref.shape[0]
    first_row = lax.axis_index("sp") * (tokens // GRID_W)
    gain = gain_ref[...]
    for c in range(tokens // HD):
        for half in range(2):
            block = 2 * c + half
            cosine, sine = table_pair(cos_ref, sin_ref, cos_ref, sin_ref, first_row + block)
            x = key_ref[GRID_W * block : GRID_W * (block + 1), :].astype(jnp.float32)
            out_ref[c, GRID_W * half : GRID_W * (half + 1), :] = turned(x, gain, cosine, sine).astype(
                jnp.bfloat16
            )
        v = value_ref[HD * c : HD * (c + 1), :].astype(jnp.float32)
        out_ref[c, HD : 2 * HD, :] = v.T.astype(jnp.bfloat16)


def q_prep_kernel(query_ref, gain_ref, cos_ref, sin_ref, out_ref):
    tokens = query_ref.shape[0]
    group = query_ref.shape[1] // HD
    first_row = lax.axis_index("sp") * (tokens // GRID_W)
    gain = gain_ref[...]
    factor = LOG2E / math.sqrt(HD)
    for pair in range(tokens // HD):
        tables = [
            table_pair(cos_ref, sin_ref, cos_ref, sin_ref, first_row + 2 * pair + half)
            for half in range(2)
        ]
        for head in range(group):
            parts = []
            for half in range(2):
                at = HD * pair + GRID_W * half
                x = query_ref[at : at + GRID_W, HD * head : HD * (head + 1)].astype(jnp.float32)
                r = turned(x, gain, *tables[half])
                parts.append(r.astype(jnp.bfloat16).astype(jnp.float32))
            flat = jnp.concatenate(parts, axis=0).T * factor
            high = flat.astype(jnp.bfloat16)
            low = (flat - high.astype(jnp.float32)).astype(jnp.bfloat16)
            column = head * tokens + HD * pair
            out_ref[0:HD, column : column + HD] = high
            out_ref[HD : 2 * HD, column : column + HD] = low


def attention_kernel(first, last, count, order_ref, qt_ref, qg_ref, kg_ref, *rest):
    kv_refs, rest = rest[:count], rest[count:]
    if first:
        state_in = None
        outs = rest
    else:
        state_in = rest[:3]
        outs = rest[3:]
    rows = 64
    places = [(ref, 2 * t) for ref in kv_refs for t in range(ref.shape[0] // 2)]
    tiles = len(places)
    columns = qt_ref.shape[1]
    if last:
        final_ref, acc_ref, sum_ref, max_ref = outs
    else:
        acc_ref, sum_ref, max_ref = outs
    bound = jnp.max(jnp.abs(qg_ref[...])) * jnp.max(jnp.abs(kg_ref[...]))
    bound = bound * (1.02 * LOG2E * math.sqrt(HD))
    safe = bound <= SAFE

    def scoped(*accs):
        scores = [[[accs[(b * 2 + m) * 4 + r] for r in range(4)] for m in range(2)] for b in range(3)]
        total = [accs[24 + m] for m in range(2)]

        def query_key(place, slot, base):
            kv_ref, block = place
            for m in range(2):
                pltpu.matmul_push_rhs(
                    qt_ref[:, pl.ds(base + 256 * m, 256)], staging_register=0, mxu_index=m
                )
            for r in range(4):
                k = kv_ref[block + r // 2, (r % 2) * rows : (r % 2 + 1) * rows, :]
                kk = jnp.concatenate([k, k], axis=1)
                for m in range(2):
                    pltpu.matmul_acc_lhs(
                        scores[slot][m][r], kk, load_staged_rhs=0 if r == 0 else None
                    )

        def weigh_values(place, slot, sums, shifts):
            kv_ref, block = place
            sums = list(sums)
            for m in range(2):
                pieces = []
                for r in range(4):
                    s = pltpu.matmul_pop(scores[slot][m][r])
                    if shifts is not None:
                        s = s - shifts[m]
                    e = jnp.exp2(s)
                    sums[m] = sums[m] + jnp.sum(e.reshape(rows // 8, 8, 256), axis=0)
                    pieces.append(e.astype(jnp.bfloat16))
                pltpu.matmul_push_rhs(
                    jnp.concatenate(pieces, axis=0), staging_register=1, mxu_index=m
                )
            v = jnp.concatenate(
                [kv_ref[block, HD : 2 * HD, :], kv_ref[block + 1, HD : 2 * HD, :]], axis=1
            )
            for m in range(2):
                pltpu.matmul_acc_lhs(total[m], v, load_staged_rhs=1)
            return tuple(sums)

        zero_sums = tuple(jnp.zeros((8, 256), jnp.float32) for _ in range(2))

        @pl.when(safe)
        def _():
            def trip(j, carry):
                base = pl.multiple_of(j * 512, 512)
                query_key(places[0], 0, base)
                query_key(places[1], 1, base)
                sums = zero_sums
                for t in range(tiles):
                    if t + 2 < tiles:
                        query_key(places[t + 2], (t + 2) % 3, base)
                    sums = weigh_values(places[t], t % 3, sums, None)
                for m in range(2):
                    at = pl.ds(base + 256 * m, 256)
                    added = pltpu.matmul_pop(total[m])
                    if state_in is None:
                        acc_ref[:, at] = added
                        sum_ref[:, at] = sums[m]
                        max_ref[:, at] = jnp.zeros((8, 256), jnp.float32)
                    else:
                        acc_ref[:, at] = state_in[0][:, at] + added
                        sum_ref[:, at] = state_in[1][:, at] + sums[m]
                        max_ref[:, at] = state_in[2][:, at]
                return carry

            lax.fori_loop(0, columns // 512, trip, 0)

        @pl.when(jnp.logical_not(safe))
        def _():
            def trip(j, carry):
                base = pl.multiple_of(j * 512, 512)
                spans = [pl.ds(base + 256 * m, 256) for m in range(2)]

                def largest(kv_ref, t, tops):
                    query_key((kv_ref, 2 * t), 0, base)
                    new = []
                    for m in range(2):
                        top = tops[m]
                        for r in range(4):
                            s = pltpu.matmul_pop(scores[0][m][r])
                            top = jnp.maximum(top, jnp.max(s.reshape(rows // 8, 8, 256), axis=0))
                        new.append(top)
                    return tuple(new)

                if state_in is None:
                    old = tuple(jnp.full((8, 256), -1e30, jnp.float32) for _ in range(2))
                else:
                    old = tuple(state_in[2][:, at] for at in spans)
                tops = old
                for ref in kv_refs:
                    tops = lax.fori_loop(
                        0, ref.shape[0] // 2, functools.partial(largest, ref), tops
                    )
                tops = [
                    jnp.broadcast_to(jnp.max(top, axis=0, keepdims=True), (8, 256)) for top in tops
                ]
                shifts = [top[0:1, :] for top in tops]

                def weigh(kv_ref, t, sums):
                    place = (kv_ref, 2 * t)
                    query_key(place, 0, base)
                    return weigh_values(place, 0, sums, shifts)

                sums = zero_sums
                for ref in kv_refs:
                    sums = lax.fori_loop(0, ref.shape[0] // 2, functools.partial(weigh, ref), sums)
                for m, at in enumerate(spans):
                    added = pltpu.matmul_pop(total[m])
                    max_ref[:, at] = tops[m]
                    if state_in is None:
                        acc_ref[:, at] = added
                        sum_ref[:, at] = sums[m]
                    else:
                        factor = jnp.exp2(old[m] - tops[m])
                        acc_ref[:, at] = state_in[0][:, at] * factor[0:1, :] + added
                        sum_ref[:, at] = state_in[1][:, at] * factor + sums[m]
                return carry

            lax.fori_loop(0, columns // 512, trip, 0)

    specs = [pltpu.ACC(m)((rows, 256), jnp.float32) for _ in range(3) for m in range(2) for _ in range(4)]
    specs += [pltpu.ACC(m)((HD, 256), jnp.float32) for m in range(2)]
    pl.run_scoped(scoped, *specs)

    if last:
        tokens = final_ref.shape[0]

        def finish(i, carry):
            for head in range(columns // tokens):
                at = pl.ds(pl.multiple_of(head * tokens + i * HD, HD), HD)
                denom = jnp.sum(sum_ref[:, at], axis=0, keepdims=True)
                block = acc_ref[:, at] / denom
                final_ref[pl.ds(pl.multiple_of(i * HD, HD), HD), head * HD : (head + 1) * HD] = (
                    block.T.astype(jnp.bfloat16)
                )
            return carry

        lax.fori_loop(0, tokens // HD, finish, 0)


def attention_chunk(order, qt, kvs, query_gain, key_gain, state, last, tokens):
    columns = qt.shape[1]
    first = state is None
    state_shapes = [
        jax.ShapeDtypeStruct((HD, columns), jnp.float32),
        jax.ShapeDtypeStruct((8, columns), jnp.float32),
        jax.ShapeDtypeStruct((8, columns), jnp.float32),
    ]
    keys = sum(kv.shape[0] for kv in kvs) * HD
    flops = 4 * columns * keys * HD
    args = [order, qt, query_gain, key_gain, *kvs] + ([] if first else list(state))
    common = dict(
        in_specs=[pl.BlockSpec(memory_space=pl.ANY)] + [vspec()] * (len(args) - 1),
        compiler_params=pltpu.CompilerParams(vmem_limit_bytes=10 << 20),
        cost_estimate=pl.CostEstimate(flops=4 * flops, bytes_accessed=keys * 4 * HD, transcendentals=0),
        name="attention",
    )
    kernel = functools.partial(attention_kernel, first, last, len(kvs))
    if last:
        return pl.pallas_call(
            kernel,
            out_shape=jax.ShapeDtypeStruct((tokens, columns // tokens * HD), jnp.bfloat16),
            out_specs=vspec(),
            scratch_shapes=[VM(s.shape, s.dtype) for s in state_shapes],
            **common,
        )(*args)
    return pl.pallas_call(
        kernel, out_shape=state_shapes, out_specs=[vspec()] * 3, **common
    )(*args)


def route_kernel(routes_ref, weight_ref, place_ref, high_ref, low_ref):
    rows, top = routes_ref.shape
    experts = place_ref.shape[0] // CAP
    slots = place_ref.shape[0]
    routes = routes_ref[...]
    weight = weight_ref[...]
    expert = lax.broadcasted_iota(jnp.int32, (rows, experts), 1)
    chosen = jnp.zeros((rows, experts), jnp.float32)
    amount = jnp.zeros((rows, experts), jnp.float32)
    for k in range(top):
        hit = routes[:, k : k + 1] == expert
        chosen = jnp.where(hit, 1.0, chosen)
        amount = jnp.where(hit, weight[:, k : k + 1], amount)
    earlier = (
        lax.broadcasted_iota(jnp.int32, (rows, rows), 0)
        > lax.broadcasted_iota(jnp.int32, (rows, rows), 1)
    ).astype(jnp.bfloat16)
    rank = jnp.dot(earlier, chosen.astype(jnp.bfloat16), preferred_element_type=jnp.float32)
    wide = (
        lax.broadcasted_iota(jnp.int32, (experts, slots), 1) // CAP
        == lax.broadcasted_iota(jnp.int32, (experts, slots), 0)
    ).astype(jnp.bfloat16)
    slot = (lax.broadcasted_iota(jnp.int32, (rows, slots), 1) % CAP).astype(jnp.float32)

    def spread(x):
        return jnp.dot(x.astype(jnp.bfloat16), wide, preferred_element_type=jnp.float32)

    mine = (spread(rank) == slot) & (spread(chosen) > 0.5)
    place_ref[...] = mine.astype(jnp.float32).T.astype(jnp.bfloat16)
    high = amount.astype(jnp.bfloat16).astype(jnp.float32)
    high_ref[...] = jnp.where(mine, spread(high), 0.0).astype(jnp.bfloat16)
    low_ref[...] = jnp.where(mine, spread(amount - high), 0.0).astype(jnp.bfloat16)


def project_kernel(
    heads_ref, weight_ref, residual_ref, gain_ref, place_ref, hidden_ref, normed_ref, send_ref
):
    parts = heads_ref.shape[0]
    depth = heads_ref.shape[2]
    total = residual_ref[...].astype(jnp.float32)
    for i in range(parts):
        total = total + jnp.dot(
            heads_ref[i], weight_ref[i * depth : (i + 1) * depth, :], preferred_element_type=jnp.float32
        )
    hidden = total.astype(jnp.bfloat16)
    hidden_ref[...] = hidden
    hidden = hidden.astype(jnp.float32)
    normed = (
        hidden
        * lax.rsqrt(jnp.mean(hidden * hidden, axis=-1, keepdims=True) + EPS)
        * gain_ref[...]
    ).astype(jnp.bfloat16)
    normed_ref[...] = normed
    step = 256

    def place(i, carry):
        at = pl.ds(pl.multiple_of(i * step, step), step)
        send_ref[at, :] = jnp.dot(
            place_ref[at, :], normed_ref[...], preferred_element_type=jnp.float32
        ).astype(jnp.bfloat16)
        return carry

    lax.fori_loop(0, send_ref.shape[0] // step, place, 0)


def expert_kernel(arrived_ref, gate_ref, up_ref, down_ref, out_ref):
    step = 256

    def block(i, carry):
        at = pl.ds(pl.multiple_of(i * step, step), step)
        x = arrived_ref[at, :]
        gate = jnp.dot(x, gate_ref[...], preferred_element_type=jnp.float32)
        up = jnp.dot(x, up_ref[...], preferred_element_type=jnp.float32)
        hidden = (jax.nn.silu(gate) * up).astype(jnp.bfloat16)
        out_ref[at, :] = jnp.dot(
            hidden, down_ref[...], preferred_element_type=jnp.float32
        ).astype(jnp.bfloat16)
        return carry

    lax.fori_loop(0, arrived_ref.shape[0] // step, block, 0)


def join_kernel(order_ref, *refs):
    out_ref = refs[-1]
    size = refs[0].shape[0]
    for i, ref in enumerate(refs[:-1]):
        out_ref[size * i : size * (i + 1)] = ref[...]


def combine_kernel(returned_ref, high_ref, low_ref, hidden_ref, normed_ref, sg_ref, su_ref, sd_ref, out_ref):
    normed = normed_ref[...]
    gate = jnp.dot(normed, sg_ref[...], preferred_element_type=jnp.float32)
    up = jnp.dot(normed, su_ref[...], preferred_element_type=jnp.float32)
    shared = (jax.nn.silu(gate) * up).astype(jnp.bfloat16)
    returned = returned_ref[...]
    total = jnp.dot(shared, sd_ref[...], preferred_element_type=jnp.float32)
    total = total + jnp.dot(high_ref[...], returned, preferred_element_type=jnp.float32)
    total = total + jnp.dot(low_ref[...], returned, preferred_element_type=jnp.float32)
    out_ref[...] = (hidden_ref[...].astype(jnp.float32) + total).astype(jnp.bfloat16)


SIDE = 4


def shifted(x, stage, step):
    pairs = []
    for z in range(SIDE):
        for y in range(SIDE):
            for core in range(2):
                move_z = (core + stage) % 2 == 0
                to_z = (z + step) % SIDE if move_z else z
                to_y = y if move_z else (y + step) % SIDE
                pairs.append(((z * SIDE + y) * 2 + core, (to_z * SIDE + to_y) * 2 + core))
    return lax.ppermute(x, "sp", pairs)


def after(x, state):
    total, sums, tops = state
    x, tops = lax.optimization_barrier((x, tops))
    return x, (total, sums, tops)


def swapped(x):
    return lax.ppermute(x, "sp", [(i, i ^ 1) for i in range(2 * SIDE * SIDE)])


def body(
    queries,
    keys,
    values,
    residual,
    out_proj,
    query_gain,
    key_gain,
    norm_gain,
    routes,
    route_weight,
    expert_gate,
    expert_up,
    expert_down,
    shared_gate,
    shared_up,
    shared_down,
):
    tokens = queries.shape[0]
    columns = queries.shape[1] // HD * tokens
    rows = residual.shape[0]
    model = residual.shape[1]
    experts = expert_gate.shape[0] * lax.axis_size("sp") * lax.axis_size("tp")
    slots = experts * CAP
    cosine, sine = (jnp.asarray(t) for t in rotary_tables())
    qg, kg = query_gain.reshape(1, HD), key_gain.reshape(1, HD)
    bf16 = jnp.bfloat16
    shape = jax.ShapeDtypeStruct
    own = pl.pallas_call(
        kv_prep_kernel,
        out_shape=shape((tokens // HD, 2 * HD, HD), bf16),
        in_specs=[vspec()] * 5,
        out_specs=vspec(),
        name="kv_prep",
    )(keys, values, kg, cosine, sine)
    cross = [[shifted(own, stage, step) for step in (1, 3, 2)] for stage in range(2)]
    qt = pl.pallas_call(
        q_prep_kernel,
        out_shape=shape((2 * HD, columns), bf16),
        in_specs=[vspec()] * 4,
        out_specs=vspec(),
        cost_estimate=pl.CostEstimate(flops=6 << 30, bytes_accessed=1 << 20, transcendentals=0),
        compiler_params=pltpu.CompilerParams(vmem_limit_bytes=56 << 20),
        name="q_prep",
    )(queries, qg, cosine, sine)
    place, high, low = pl.pallas_call(
        route_kernel,
        out_shape=[shape((slots, rows), bf16), shape((rows, slots), bf16), shape((rows, slots), bf16)],
        in_specs=[vspec()] * 2,
        out_specs=[vspec()] * 3,
        cost_estimate=pl.CostEstimate(flops=2 << 30, bytes_accessed=1 << 20, transcendentals=0),
        compiler_params=pltpu.CompilerParams(vmem_limit_bytes=8 << 20),
        name="route",
    )(routes, route_weight)

    def attend(kvs, state, last=False, order=query_gain):
        return attention_chunk(order, qt, kvs, qg, kg, state, last, tokens)

    def join(pieces):
        return pl.pallas_call(
            join_kernel,
            out_shape=shape((len(pieces) * own.shape[0],) + own.shape[1:], bf16),
            in_specs=[pl.BlockSpec(memory_space=pl.ANY)] + [vspec()] * len(pieces),
            out_specs=vspec(),
            compiler_params=pltpu.CompilerParams(vmem_limit_bytes=6 << 20),
            name="join",
        )(qt, *pieces)

    ring = join(cross[0])
    far = [shifted(ring, 1, step) for step in (1, 3, 2)]
    side = join(cross[1])
    near = [own, ring, side]
    near_twins = [swapped(kv) for kv in near]
    state = attend(near, None)
    state = attend(near_twins, state)
    far[0], state = after(far[0], state)
    twin = swapped(far[0])
    state = attend([far[0]], state, order=place)
    far[1], state = after(far[1], state)
    twin, before = swapped(far[1]), twin
    state = attend([before, far[1]], state)
    far[2], state = after(far[2], state)
    twin, before = swapped(far[2]), twin
    state = attend([before, far[2]], state)
    attn_local = attend([twin], state, True)
    parts = tokens // rows
    all_heads = lax.all_to_all(
        attn_local.reshape(parts, rows, attn_local.shape[1]), "tp", split_axis=0, concat_axis=0, tiled=True
    )
    hidden1, normed, send = pl.pallas_call(
        project_kernel,
        out_shape=[shape((rows, model), bf16), shape((rows, model), bf16), shape((slots, model), bf16)],
        in_specs=[vspec()] * 5,
        out_specs=[vspec()] * 3,
        compiler_params=pltpu.CompilerParams(vmem_limit_bytes=16 << 20),
        name="project",
    )(all_heads, out_proj, residual, norm_gain.reshape(1, model), place)
    arrived = lax.all_to_all(
        send.reshape(experts, CAP, model), ("sp", "tp"), split_axis=0, concat_axis=0, tiled=True
    ).reshape(slots, model)
    processed = pl.pallas_call(
        expert_kernel,
        out_shape=shape((slots, model), bf16),
        in_specs=[vspec()] * 4,
        out_specs=vspec(),
        compiler_params=pltpu.CompilerParams(vmem_limit_bytes=24 << 20),
        name="experts",
    )(arrived, expert_gate[0], expert_up[0], expert_down[0])
    returned = lax.all_to_all(
        processed.reshape(experts, CAP, model), ("sp", "tp"), split_axis=0, concat_axis=0, tiled=True
    ).reshape(slots, model)
    return pl.pallas_call(
        combine_kernel,
        out_shape=shape((rows, model), bf16),
        in_specs=[vspec()] * 8,
        out_specs=vspec(),
        compiler_params=pltpu.CompilerParams(vmem_limit_bytes=16 << 20),
        name="combine",
    )(returned, high, low, hidden1, normed, shared_gate, shared_up, shared_down)


def solution(mesh):
    placed = (
        P("sp", "tp"),
        P("sp", "tp"),
        P("sp", "tp"),
        P(("sp", "tp"), None),
        P(),
        P(),
        P(),
        P(),
        P(("sp", "tp"), None),
        P(("sp", "tp"), None),
        P(("sp", "tp"), None, None),
        P(("sp", "tp"), None, None),
        P(("sp", "tp"), None, None),
        P(),
        P(),
        P(),
    )
    return jax.shard_map(
        body, mesh=mesh, in_specs=placed, out_specs=P(("sp", "tp"), None), check_vma=False
    )
```

```python
import functools
import math

import jax
import jax.numpy as jnp
import numpy as np
from jax import lax
from jax.experimental import pallas as pl
from jax.experimental.pallas import tpu as pltpu
from jax.sharding import Mesh
from jax.sharding import PartitionSpec as P

HEADS = 16
KV_HEADS = 4
GRID_W = 64
HD = 128
CAP = 8
EPS = 1e-06
THETA = 10000.0
LOG2E = math.log2(math.e)
SAFE = 80.0
VM = pltpu.VMEM


def vspec():
    return pl.BlockSpec(memory_space=VM)


def rotary_tables():
    quarter = HD // 4
    inverse = np.power(THETA, -4.0 * np.arange(quarter, dtype=np.float64) / HD).astype(np.float32)
    angles = (np.arange(256, dtype=np.float32)[:, None] * inverse[None, :]).astype(np.float64)
    cos, sin = np.cos(angles), np.sin(angles)
    cosine = np.concatenate([cos, cos, cos, cos], axis=1).astype(np.float32)
    sine = np.concatenate([-sin, sin, -sin, sin], axis=1).astype(np.float32)
    return cosine, sine


def turned(x, gain, cosine, sine):
    x = x * lax.rsqrt(jnp.mean(x * x, axis=-1, keepdims=True) + EPS) * gain
    lane = lax.broadcasted_iota(jnp.int32, x.shape, 1)
    partner = jnp.where((lane // 32) % 2 == 0, pltpu.roll(x, 96, 1), pltpu.roll(x, 32, 1))
    return x * cosine + partner * sine


def table_pair(row_cos, row_sin, col_cos, col_sin, row):
    lane = lax.broadcasted_iota(jnp.int32, (GRID_W, HD), 1)
    cosine = jnp.where(lane < 64, row_cos[pl.ds(row, 1), :], col_cos[0:GRID_W, :])
    sine = jnp.where(lane < 64, row_sin[pl.ds(row, 1), :], col_sin[0:GRID_W, :])
    return cosine, sine


def kv_prep_kernel(key_ref, value_ref, gain_ref, cos_ref, sin_ref, out_ref):
    tokens = key_ref.shape[0]
    first_row = lax.axis_index("sp") * (tokens // GRID_W)
    gain = gain_ref[...]
    for c in range(tokens // HD):
        for half in range(2):
            block = 2 * c + half
            cosine, sine = table_pair(cos_ref, sin_ref, cos_ref, sin_ref, first_row + block)
            x = key_ref[GRID_W * block : GRID_W * (block + 1), :].astype(jnp.float32)
            out_ref[c, GRID_W * half : GRID_W * (half + 1), :] = turned(x, gain, cosine, sine).astype(
                jnp.bfloat16
            )
        v = value_ref[HD * c : HD * (c + 1), :].astype(jnp.float32)
        out_ref[c, HD : 2 * HD, :] = v.T.astype(jnp.bfloat16)


def q_prep_kernel(query_ref, gain_ref, cos_ref, sin_ref, out_ref, done_ref):
    tokens = query_ref.shape[0]
    group = query_ref.shape[1] // HD
    first_row = lax.axis_index("sp") * (tokens // GRID_W)
    gain = jnp.broadcast_to(gain_ref[...], (HD, HD)).T
    factor = LOG2E / math.sqrt(HD)
    quarter = HD // 4
    for pair in range(tokens // HD):
        tables = [
            table_pair(cos_ref, sin_ref, cos_ref, sin_ref, first_row + 2 * pair + half)
            for half in range(2)
        ]
        cosine, sine = (jnp.concatenate([tables[0][i], tables[1][i]], axis=0).T for i in range(2))
        for head in range(group):
            x = query_ref[HD * pair : HD * (pair + 1), HD * head : HD * (head + 1)]
            x = x.astype(jnp.float32).T
            x = x * lax.rsqrt(jnp.mean(x * x, axis=0, keepdims=True) + EPS) * gain
            partner = jnp.concatenate(
                [x[quarter * i : quarter * (i + 1)] for i in (1, 0, 3, 2)], axis=0
            )
            rounded = (x * cosine + partner * sine).astype(jnp.bfloat16)
            scaled = rounded.astype(jnp.float32) * factor
            high = scaled.astype(jnp.bfloat16)
            low = (scaled - high.astype(jnp.float32)).astype(jnp.bfloat16)
            column = HD * (group * pair + head)
            out_ref[0:HD, column : column + HD] = high
            out_ref[HD : 2 * HD, column : column + HD] = low
    done_ref[...] = jnp.zeros_like(done_ref)


def attention_kernel(first, steps, count, order_ref, qt_ref, qg_ref, kg_ref, *rest):
    kv_refs, rest = rest[:count], rest[count:]
    if first:
        state_in = None
        outs = rest
    else:
        state_in = rest[:3]
        outs = rest[3:]
    rows = 64
    places = [(ref, 2 * t) for ref in kv_refs for t in range(ref.shape[0] // 2)]
    tiles = len(places)
    columns = qt_ref.shape[1]
    final_refs, (acc_ref, sum_ref, max_ref) = outs[:-3], outs[-3:]
    start, trips = 0, columns // 512
    if steps:
        start, trips = lax.axis_index("tp") + steps[0], len(steps)
    bound = jnp.max(jnp.abs(qg_ref[...])) * jnp.max(jnp.abs(kg_ref[...]))
    bound = bound * (1.02 * LOG2E * math.sqrt(HD))
    safe = bound <= SAFE

    def scoped(*accs):
        scores = [[[accs[(b * 2 + m) * 4 + r] for r in range(4)] for m in range(2)] for b in range(3)]
        total = [accs[24 + m] for m in range(2)]

        def query_key(place, slot, base):
            kv_ref, block = place
            for m in range(2):
                pltpu.matmul_push_rhs(
                    qt_ref[:, pl.ds(base + 256 * m, 256)], staging_register=0, mxu_index=m
                )
            for r in range(4):
                k = kv_ref[block + r // 2, (r % 2) * rows : (r % 2 + 1) * rows, :]
                kk = jnp.concatenate([k, k], axis=1)
                for m in range(2):
                    pltpu.matmul_acc_lhs(
                        scores[slot][m][r], kk, load_staged_rhs=0 if r == 0 else None
                    )

        def weigh_values(place, slot, sums, shifts):
            kv_ref, block = place
            sums = list(sums)
            for m in range(2):
                pieces = []
                for r in range(4):
                    s = pltpu.matmul_pop(scores[slot][m][r])
                    if shifts is not None:
                        s = s - shifts[m]
                    e = jnp.exp2(s)
                    sums[m] = sums[m] + jnp.sum(e.reshape(rows // 8, 8, 256), axis=0)
                    pieces.append(e.astype(jnp.bfloat16))
                pltpu.matmul_push_rhs(
                    jnp.concatenate(pieces, axis=0), staging_register=1, mxu_index=m
                )
            v = jnp.concatenate(
                [kv_ref[block, HD : 2 * HD, :], kv_ref[block + 1, HD : 2 * HD, :]], axis=1
            )
            for m in range(2):
                pltpu.matmul_acc_lhs(total[m], v, load_staged_rhs=1)
            return tuple(sums)

        zero_sums = tuple(jnp.zeros((8, 256), jnp.float32) for _ in range(2))

        @pl.when(safe)
        def _():
            def trip(j, carry):
                base = pl.multiple_of(lax.rem(start + j, columns // 512) * 512, 512)
                query_key(places[0], 0, base)
                query_key(places[1], 1, base)
                sums = zero_sums
                for t in range(tiles):
                    if t + 2 < tiles:
                        query_key(places[t + 2], (t + 2) % 3, base)
                    sums = weigh_values(places[t], t % 3, sums, None)
                for m in range(2):
                    at = pl.ds(base + 256 * m, 256)
                    added = pltpu.matmul_pop(total[m])
                    if state_in is None:
                        acc_ref[:, at] = added
                        sum_ref[:, at] = sums[m]
                        max_ref[:, at] = jnp.zeros((8, 256), jnp.float32)
                    else:
                        acc_ref[:, at] = state_in[0][:, at] + added
                        sum_ref[:, at] = state_in[1][:, at] + sums[m]
                        max_ref[:, at] = state_in[2][:, at]
                return carry

            lax.fori_loop(0, trips, trip, 0)

        @pl.when(jnp.logical_not(safe))
        def _():
            def trip(j, carry):
                base = pl.multiple_of(lax.rem(start + j, columns // 512) * 512, 512)
                spans = [pl.ds(base + 256 * m, 256) for m in range(2)]

                def largest(kv_ref, t, tops):
                    query_key((kv_ref, 2 * t), 0, base)
                    new = []
                    for m in range(2):
                        top = tops[m]
                        for r in range(4):
                            s = pltpu.matmul_pop(scores[0][m][r])
                            top = jnp.maximum(top, jnp.max(s.reshape(rows // 8, 8, 256), axis=0))
                        new.append(top)
                    return tuple(new)

                if state_in is None:
                    old = tuple(jnp.full((8, 256), -1e30, jnp.float32) for _ in range(2))
                else:
                    old = tuple(state_in[2][:, at] for at in spans)
                tops = old
                for ref in kv_refs:
                    tops = lax.fori_loop(
                        0, ref.shape[0] // 2, functools.partial(largest, ref), tops
                    )
                tops = [
                    jnp.broadcast_to(jnp.max(top, axis=0, keepdims=True), (8, 256)) for top in tops
                ]
                shifts = [top[0:1, :] for top in tops]

                def weigh(kv_ref, t, sums):
                    place = (kv_ref, 2 * t)
                    query_key(place, 0, base)
                    return weigh_values(place, 0, sums, shifts)

                sums = zero_sums
                for ref in kv_refs:
                    sums = lax.fori_loop(0, ref.shape[0] // 2, functools.partial(weigh, ref), sums)
                for m, at in enumerate(spans):
                    added = pltpu.matmul_pop(total[m])
                    max_ref[:, at] = tops[m]
                    if state_in is None:
                        acc_ref[:, at] = added
                        sum_ref[:, at] = sums[m]
                    else:
                        factor = jnp.exp2(old[m] - tops[m])
                        acc_ref[:, at] = state_in[0][:, at] * factor[0:1, :] + added
                        sum_ref[:, at] = state_in[1][:, at] * factor + sums[m]
                return carry

            lax.fori_loop(0, trips, trip, 0)

    specs = [pltpu.ACC(m)((rows, 256), jnp.float32) for _ in range(3) for m in range(2) for _ in range(4)]
    specs += [pltpu.ACC(m)((HD, 256), jnp.float32) for m in range(2)]
    pl.run_scoped(scoped, *specs)

    for step, final_ref in enumerate(final_refs):
        base = lax.rem(start + step, columns // 512) * 512
        for head in range(512 // HD):
            at = pl.ds(pl.multiple_of(base + head * HD, HD), HD)
            denom = jnp.sum(sum_ref[:, at], axis=0, keepdims=True)
            block = acc_ref[:, at] / denom
            final_ref[:, head * HD : (head + 1) * HD] = block.T.astype(jnp.bfloat16)


def attention_chunk(order, qt, kvs, query_gain, key_gain, state, steps):
    columns = qt.shape[1]
    first = state is None
    state_shapes = [
        jax.ShapeDtypeStruct((HD, columns), jnp.float32),
        jax.ShapeDtypeStruct((8, columns), jnp.float32),
        jax.ShapeDtypeStruct((8, columns), jnp.float32),
    ]
    keys = sum(kv.shape[0] for kv in kvs) * HD
    flops = 4 * columns * keys * HD // (2 if steps else 1)
    args = [order, qt, query_gain, key_gain, *kvs] + ([] if first else list(state))
    common = dict(
        in_specs=[pl.BlockSpec(memory_space=pl.ANY)] + [vspec()] * (len(args) - 1),
        compiler_params=pltpu.CompilerParams(vmem_limit_bytes=10 << 20),
        cost_estimate=pl.CostEstimate(flops=4 * flops, bytes_accessed=keys * 4 * HD, transcendentals=0),
        name="attention",
    )
    kernel = functools.partial(attention_kernel, first, steps, len(kvs))
    if steps:
        return pl.pallas_call(
            kernel,
            out_shape=[jax.ShapeDtypeStruct((HD, 512), jnp.bfloat16)] * len(steps),
            out_specs=[vspec()] * len(steps),
            scratch_shapes=[VM(s.shape, s.dtype) for s in state_shapes],
            **common,
        )(*args)
    return pl.pallas_call(
        kernel, out_shape=state_shapes, out_specs=[vspec()] * 3, **common
    )(*args)


def route_kernel(routes_ref, weight_ref, place_ref, mix_ref):
    rows, top = routes_ref.shape
    experts = place_ref.shape[0] // CAP
    slots = place_ref.shape[0]
    routes = routes_ref[...]
    weight = weight_ref[...]
    expert = lax.broadcasted_iota(jnp.int32, (rows, experts), 1)
    chosen = jnp.zeros((rows, experts), jnp.float32)
    amount = jnp.zeros((rows, experts), jnp.float32)
    for k in range(top):
        hit = routes[:, k : k + 1] == expert
        chosen = jnp.where(hit, 1.0, chosen)
        amount = jnp.where(hit, weight[:, k : k + 1], amount)
    earlier = (
        lax.broadcasted_iota(jnp.int32, (rows, rows), 0)
        > lax.broadcasted_iota(jnp.int32, (rows, rows), 1)
    ).astype(jnp.bfloat16)
    rank = jnp.dot(earlier, chosen.astype(jnp.bfloat16), preferred_element_type=jnp.float32)
    wide = (
        lax.broadcasted_iota(jnp.int32, (experts, slots), 1) // CAP
        == lax.broadcasted_iota(jnp.int32, (experts, slots), 0)
    ).astype(jnp.bfloat16)
    slot = (lax.broadcasted_iota(jnp.int32, (rows, slots), 1) % CAP).astype(jnp.float32)

    def spread(x):
        return jnp.dot(x.astype(jnp.bfloat16), wide, preferred_element_type=jnp.float32)

    mine = (spread(rank) == slot) & (spread(chosen) > 0.5)
    place_ref[...] = mine.astype(jnp.float32).T.astype(jnp.bfloat16)
    high = amount.astype(jnp.bfloat16).astype(jnp.float32)
    mix_ref[0:rows, :] = jnp.where(mine, spread(high), 0.0).astype(jnp.bfloat16)
    mix_ref[rows:, :] = jnp.where(mine, spread(amount - high), 0.0).astype(jnp.bfloat16)


def project_kernel(parts, *refs):
    head_refs = refs[:parts]
    weight_ref, residual_ref, gain_ref, place_ref, hidden_ref, normed_ref, send_ref = refs[parts:]
    depth = head_refs[0].shape[1]
    me = lax.axis_index("tp")
    total = residual_ref[...].astype(jnp.float32)
    for step, head_ref in enumerate(head_refs):
        part = lax.rem(me + parts - step, parts)
        weight = weight_ref[pl.ds(pl.multiple_of(part * depth, depth), depth), :]
        total = total + jnp.dot(head_ref[...], weight, preferred_element_type=jnp.float32)
    hidden = total.astype(jnp.bfloat16)
    hidden_ref[...] = hidden
    hidden = hidden.astype(jnp.float32)
    normed_ref[...] = (
        hidden
        * lax.rsqrt(jnp.mean(hidden * hidden, axis=-1, keepdims=True) + EPS)
        * gain_ref[...]
    ).astype(jnp.bfloat16)
    step = 256

    def place(i, carry):
        at = pl.ds(pl.multiple_of(i * step, step), step)
        send_ref[at, :] = jnp.dot(
            place_ref[at, :], normed_ref[...], preferred_element_type=jnp.float32
        ).astype(jnp.bfloat16)
        return carry

    lax.fori_loop(0, send_ref.shape[0] // step, place, 0)


def expert_kernel(arrived_ref, gate_ref, up_ref, down_ref, out_ref):
    step = 512

    def block(i, carry):
        at = pl.ds(pl.multiple_of(i * step, step), step)
        x = arrived_ref[at, :]
        gate = jnp.dot(x, gate_ref[...], preferred_element_type=jnp.float32)
        up = jnp.dot(x, up_ref[...], preferred_element_type=jnp.float32)
        hidden = (jax.nn.silu(gate) * up).astype(jnp.bfloat16)
        out_ref[at, :] = jnp.dot(
            hidden, down_ref[...], preferred_element_type=jnp.float32
        ).astype(jnp.bfloat16)
        return carry

    lax.fori_loop(0, arrived_ref.shape[0] // step, block, 0)


def join_kernel(order_ref, *refs):
    out_ref = refs[-1]
    size = refs[0].shape[0]
    for i, ref in enumerate(refs[:-1]):
        out_ref[size * i : size * (i + 1)] = ref[...]


def combine_kernel(returned_ref, mix_ref, hidden_ref, normed_ref, sg_ref, su_ref, sd_ref, out_ref):
    normed = normed_ref[...]
    gate = jnp.dot(normed, sg_ref[...], preferred_element_type=jnp.float32)
    up = jnp.dot(normed, su_ref[...], preferred_element_type=jnp.float32)
    shared = (jax.nn.silu(gate) * up).astype(jnp.bfloat16)
    returned = returned_ref[...]
    total = jnp.dot(shared, sd_ref[...], preferred_element_type=jnp.float32)
    routed = jnp.dot(mix_ref[...], returned, preferred_element_type=jnp.float32)
    rows = total.shape[0]
    total = total + (routed[0:rows] + routed[rows:])
    out_ref[...] = (hidden_ref[...].astype(jnp.float32) + total).astype(jnp.bfloat16)


SIDE = 4


def shifted(x, stage, step):
    pairs = []
    for z in range(SIDE):
        for y in range(SIDE):
            for core in range(2):
                move_z = (core + stage) % 2 == 0
                to_z = (z + step) % SIDE if move_z else z
                to_y = y if move_z else (y + step) % SIDE
                pairs.append(((z * SIDE + y) * 2 + core, (to_z * SIDE + to_y) * 2 + core))
    return lax.ppermute(x, "sp", pairs)


def after(x, state):
    total, sums, tops = state
    *x, tops = lax.optimization_barrier((*x, tops))
    return x, (total, sums, tops)


def swapped(x):
    return lax.ppermute(x, "sp", [(i, i ^ 1) for i in range(2 * SIDE * SIDE)])


def body(
    queries,
    keys,
    values,
    residual,
    out_proj,
    query_gain,
    key_gain,
    norm_gain,
    routes,
    route_weight,
    expert_gate,
    expert_up,
    expert_down,
    shared_gate,
    shared_up,
    shared_down,
):
    tokens = queries.shape[0]
    columns = queries.shape[1] // HD * tokens
    rows = residual.shape[0]
    model = residual.shape[1]
    experts = expert_gate.shape[0] * lax.axis_size("sp") * lax.axis_size("tp")
    slots = experts * CAP
    cosine, sine = (jnp.asarray(t) for t in rotary_tables())
    qg, kg = query_gain.reshape(1, HD), key_gain.reshape(1, HD)
    bf16 = jnp.bfloat16
    shape = jax.ShapeDtypeStruct
    own = pl.pallas_call(
        kv_prep_kernel,
        out_shape=shape((tokens // HD, 2 * HD, HD), bf16),
        in_specs=[vspec()] * 5,
        out_specs=vspec(),
        name="kv_prep",
    )(keys, values, kg, cosine, sine)
    pieces = [shifted(own, 0, step) for step in (1, 3, 2)]
    qt, q_done = pl.pallas_call(
        q_prep_kernel,
        out_shape=[shape((2 * HD, columns), bf16), shape((8, HD), jnp.float32)],
        in_specs=[vspec()] * 4,
        out_specs=[vspec()] * 2,
        cost_estimate=pl.CostEstimate(flops=6 << 30, bytes_accessed=1 << 20, transcendentals=0),
        compiler_params=pltpu.CompilerParams(vmem_limit_bytes=56 << 20),
        name="q_prep",
    )(queries, qg, cosine, sine)
    place, mix = pl.pallas_call(
        route_kernel,
        out_shape=[shape((slots, rows), bf16), shape((2 * rows, slots), bf16)],
        in_specs=[vspec()] * 2,
        out_specs=[vspec()] * 2,
        cost_estimate=pl.CostEstimate(flops=2 << 30, bytes_accessed=1 << 20, transcendentals=0),
        compiler_params=pltpu.CompilerParams(vmem_limit_bytes=8 << 20),
        name="route",
    )(routes, route_weight)

    def attend(kvs, state, steps=(), order=query_gain):
        return attention_chunk(order, qt, kvs, qg, kg, state, steps)

    def join(pieces):
        return pl.pallas_call(
            join_kernel,
            out_shape=shape((len(pieces) * own.shape[0],) + own.shape[1:], bf16),
            in_specs=[pl.BlockSpec(memory_space=pl.ANY)] + [vspec()] * len(pieces),
            out_specs=vspec(),
            compiler_params=pltpu.CompilerParams(vmem_limit_bytes=6 << 20),
            name="join",
        )(q_done, *pieces)

    first, second = join([own, pieces[0]]), join(pieces[1:])
    up1, down2 = shifted(first, 1, 1), shifted(second, 1, 3)
    up2, down1 = shifted(second, 1, 1), shifted(first, 1, 3)
    twins = [swapped(first), swapped(second)]
    state = attend([first, second], None)
    state = attend(twins, state)
    (up1, down2), state = after([up1, down2], state)
    far1, far2 = shifted(up1, 1, 1), shifted(down2, 1, 3)
    twins = [swapped(up1), swapped(down2)]
    state = attend([up1, down2], state, order=place)
    (up2, down1), state = after([up2, down1], state)
    more = [swapped(up2), swapped(down1)]
    state = attend([*twins, up2, down1], state)
    (far1, far2), state = after([far1, far2], state)
    last = [swapped(far1), swapped(far2)]
    state = attend([*more, far1, far2], state)
    parts = columns // 512

    def exchanged(piece, step):
        return lax.ppermute(piece, "tp", [(i, (i + step) % parts) for i in range(parts)])

    one, two = attend(last, state, (1, 2))
    two, one = exchanged(two, 2), exchanged(one, 1)
    three, none = attend(last, state, (3, 4))
    heads = [none, one, two, exchanged(three, 3)]
    hidden1, normed, send = pl.pallas_call(
        functools.partial(project_kernel, parts),
        out_shape=[shape((rows, model), bf16), shape((rows, model), bf16), shape((slots, model), bf16)],
        in_specs=[vspec()] * (parts + 4),
        out_specs=[vspec()] * 3,
        compiler_params=pltpu.CompilerParams(vmem_limit_bytes=16 << 20),
        name="project",
    )(*heads, out_proj, residual, norm_gain.reshape(1, model), place)
    arrived = lax.all_to_all(
        send.reshape(experts, CAP, model), ("sp", "tp"), split_axis=0, concat_axis=0, tiled=True
    ).reshape(slots, model)
    processed = pl.pallas_call(
        expert_kernel,
        out_shape=shape((slots, model), bf16),
        in_specs=[vspec()] * 4,
        out_specs=vspec(),
        compiler_params=pltpu.CompilerParams(vmem_limit_bytes=24 << 20),
        name="experts",
    )(arrived, expert_gate[0], expert_up[0], expert_down[0])
    returned = lax.all_to_all(
        processed.reshape(experts, CAP, model), ("sp", "tp"), split_axis=0, concat_axis=0, tiled=True
    ).reshape(slots, model)
    return pl.pallas_call(
        combine_kernel,
        out_shape=shape((rows, model), bf16),
        in_specs=[vspec()] * 7,
        out_specs=vspec(),
        compiler_params=pltpu.CompilerParams(vmem_limit_bytes=16 << 20),
        name="combine",
    )(returned, mix, hidden1, normed, shared_gate, shared_up, shared_down)


def solution(mesh):
    placed = (
        P("sp", "tp"),
        P("sp", "tp"),
        P("sp", "tp"),
        P(("sp", "tp"), None),
        P(),
        P(),
        P(),
        P(),
        P(("sp", "tp"), None),
        P(("sp", "tp"), None),
        P(("sp", "tp"), None, None),
        P(("sp", "tp"), None, None),
        P(("sp", "tp"), None, None),
        P(),
        P(),
        P(),
    )
    return jax.shard_map(
        body, mesh=mesh, in_specs=placed, out_specs=P(("sp", "tp"), None), check_vma=False
    )
```

```python
import functools
import math

import jax
import jax.numpy as jnp
import numpy as np
from jax import lax
from jax.experimental import pallas as pl
from jax.experimental.pallas import tpu as pltpu
from jax.sharding import Mesh
from jax.sharding import PartitionSpec as P

HEADS = 16
KV_HEADS = 4
GRID_W = 64
HD = 128
CAP = 8
EPS = 1e-06
THETA = 10000.0
LOG2E = math.log2(math.e)
SAFE = 80.0
VM = pltpu.VMEM


def vspec():
    return pl.BlockSpec(memory_space=VM)


def rotary_tables():
    quarter = HD // 4
    inverse = np.power(THETA, -4.0 * np.arange(quarter, dtype=np.float64) / HD).astype(np.float32)
    angles = (np.arange(256, dtype=np.float32)[:, None] * inverse[None, :]).astype(np.float64)
    cos, sin = np.cos(angles), np.sin(angles)
    cosine = np.concatenate([cos, cos, cos, cos], axis=1).astype(np.float32)
    sine = np.concatenate([-sin, sin, -sin, sin], axis=1).astype(np.float32)
    return cosine, sine


def turned(x, gain, cosine, sine):
    x = x * lax.rsqrt(jnp.mean(x * x, axis=-1, keepdims=True) + EPS) * gain
    lane = lax.broadcasted_iota(jnp.int32, x.shape, 1)
    partner = jnp.where((lane // 32) % 2 == 0, pltpu.roll(x, 96, 1), pltpu.roll(x, 32, 1))
    return x * cosine + partner * sine


def table_pair(row_cos, row_sin, col_cos, col_sin, row):
    lane = lax.broadcasted_iota(jnp.int32, (GRID_W, HD), 1)
    cosine = jnp.where(lane < 64, row_cos[pl.ds(row, 1), :], col_cos[0:GRID_W, :])
    sine = jnp.where(lane < 64, row_sin[pl.ds(row, 1), :], col_sin[0:GRID_W, :])
    return cosine, sine


def kv_prep_kernel(key_ref, value_ref, gain_ref, cos_ref, sin_ref, out_ref):
    tokens = key_ref.shape[0]
    first_row = lax.axis_index("sp") * (tokens // GRID_W)
    gain = gain_ref[...]
    for c in range(tokens // HD):
        for half in range(2):
            block = 2 * c + half
            cosine, sine = table_pair(cos_ref, sin_ref, cos_ref, sin_ref, first_row + block)
            x = key_ref[GRID_W * block : GRID_W * (block + 1), :].astype(jnp.float32)
            out_ref[c, GRID_W * half : GRID_W * (half + 1), :] = turned(x, gain, cosine, sine).astype(
                jnp.bfloat16
            )
        v = value_ref[HD * c : HD * (c + 1), :].astype(jnp.float32)
        out_ref[c, HD : 2 * HD, :] = v.T.astype(jnp.bfloat16)


def q_prep_kernel(query_ref, gain_ref, cos_ref, sin_ref, out_ref, done_ref):
    tokens = query_ref.shape[0]
    group = query_ref.shape[1] // HD
    first_row = lax.axis_index("sp") * (tokens // GRID_W)
    gain = jnp.broadcast_to(gain_ref[...], (HD, HD)).T
    factor = LOG2E / math.sqrt(HD)
    quarter = HD // 4
    for pair in range(tokens // HD):
        tables = [
            table_pair(cos_ref, sin_ref, cos_ref, sin_ref, first_row + 2 * pair + half)
            for half in range(2)
        ]
        cosine, sine = (jnp.concatenate([tables[0][i], tables[1][i]], axis=0).T for i in range(2))
        for head in range(group):
            x = query_ref[HD * pair : HD * (pair + 1), HD * head : HD * (head + 1)]
            x = x.astype(jnp.float32).T
            x = x * lax.rsqrt(jnp.mean(x * x, axis=0, keepdims=True) + EPS) * gain
            partner = jnp.concatenate(
                [x[quarter * i : quarter * (i + 1)] for i in (1, 0, 3, 2)], axis=0
            )
            rounded = (x * cosine + partner * sine).astype(jnp.bfloat16)
            scaled = rounded.astype(jnp.float32) * factor
            high = scaled.astype(jnp.bfloat16)
            low = (scaled - high.astype(jnp.float32)).astype(jnp.bfloat16)
            column = HD * (group * pair + head)
            out_ref[0:HD, column : column + HD] = high
            out_ref[HD : 2 * HD, column : column + HD] = low
    done_ref[...] = jnp.zeros_like(done_ref)


def attention_kernel(first, steps, count, order_ref, qt_ref, qg_ref, kg_ref, *rest):
    kv_refs, rest = rest[:count], rest[count:]
    if first:
        state_in = None
        outs = rest
    else:
        state_in = rest[:3]
        outs = rest[3:]
    rows = 64
    places = [(ref, 2 * t) for ref in kv_refs for t in range(ref.shape[0] // 2)]
    tiles = len(places)
    columns = qt_ref.shape[1]
    final_refs, (acc_ref, sum_ref, max_ref) = outs[:-3], outs[-3:]
    start, trips = 0, columns // 512
    if steps:
        start, trips = lax.axis_index("tp") + steps[0], len(steps)
    bound = jnp.max(jnp.abs(qg_ref[...])) * jnp.max(jnp.abs(kg_ref[...]))
    bound = bound * (1.02 * LOG2E * math.sqrt(HD))
    safe = bound <= SAFE

    def scoped(*accs):
        scores = [[[accs[(b * 2 + m) * 4 + r] for r in range(4)] for m in range(2)] for b in range(3)]
        total = [accs[24 + m] for m in range(2)]

        def query_key(place, slot, base):
            kv_ref, block = place
            for m in range(2):
                pltpu.matmul_push_rhs(
                    qt_ref[:, pl.ds(base + 256 * m, 256)], staging_register=0, mxu_index=m
                )
            for r in range(4):
                k = kv_ref[block + r // 2, (r % 2) * rows : (r % 2 + 1) * rows, :]
                kk = jnp.concatenate([k, k], axis=1)
                for m in range(2):
                    pltpu.matmul_acc_lhs(
                        scores[slot][m][r], kk, load_staged_rhs=0 if r == 0 else None
                    )

        def weigh_values(place, slot, sums, shifts):
            kv_ref, block = place
            sums = list(sums)
            for m in range(2):
                pieces = []
                for r in range(4):
                    s = pltpu.matmul_pop(scores[slot][m][r])
                    if shifts is not None:
                        s = s - shifts[m]
                    e = jnp.exp2(s)
                    sums[m] = sums[m] + jnp.sum(e.reshape(rows // 8, 8, 256), axis=0)
                    pieces.append(e.astype(jnp.bfloat16))
                pltpu.matmul_push_rhs(
                    jnp.concatenate(pieces, axis=0), staging_register=1, mxu_index=m
                )
            v = jnp.concatenate(
                [kv_ref[block, HD : 2 * HD, :], kv_ref[block + 1, HD : 2 * HD, :]], axis=1
            )
            for m in range(2):
                pltpu.matmul_acc_lhs(total[m], v, load_staged_rhs=1)
            return tuple(sums)

        zero_sums = tuple(jnp.zeros((8, 256), jnp.float32) for _ in range(2))

        @pl.when(safe)
        def _():
            def trip(j, carry):
                base = pl.multiple_of(lax.rem(start + j, columns // 512) * 512, 512)
                query_key(places[0], 0, base)
                query_key(places[1], 1, base)
                sums = zero_sums
                for t in range(tiles):
                    if t + 2 < tiles:
                        query_key(places[t + 2], (t + 2) % 3, base)
                    sums = weigh_values(places[t], t % 3, sums, None)
                for m in range(2):
                    at = pl.ds(base + 256 * m, 256)
                    added = pltpu.matmul_pop(total[m])
                    if state_in is None:
                        acc_ref[:, at] = added
                        sum_ref[:, at] = sums[m]
                        max_ref[:, at] = jnp.zeros((8, 256), jnp.float32)
                    else:
                        acc_ref[:, at] = state_in[0][:, at] + added
                        sum_ref[:, at] = state_in[1][:, at] + sums[m]
                        max_ref[:, at] = state_in[2][:, at]
                return carry

            lax.fori_loop(0, trips, trip, 0)

        @pl.when(jnp.logical_not(safe))
        def _():
            def trip(j, carry):
                base = pl.multiple_of(lax.rem(start + j, columns // 512) * 512, 512)
                spans = [pl.ds(base + 256 * m, 256) for m in range(2)]

                def largest(kv_ref, t, tops):
                    query_key((kv_ref, 2 * t), 0, base)
                    new = []
                    for m in range(2):
                        top = tops[m]
                        for r in range(4):
                            s = pltpu.matmul_pop(scores[0][m][r])
                            top = jnp.maximum(top, jnp.max(s.reshape(rows // 8, 8, 256), axis=0))
                        new.append(top)
                    return tuple(new)

                if state_in is None:
                    old = tuple(jnp.full((8, 256), -1e30, jnp.float32) for _ in range(2))
                else:
                    old = tuple(state_in[2][:, at] for at in spans)
                tops = old
                for ref in kv_refs:
                    tops = lax.fori_loop(
                        0, ref.shape[0] // 2, functools.partial(largest, ref), tops
                    )
                tops = [
                    jnp.broadcast_to(jnp.max(top, axis=0, keepdims=True), (8, 256)) for top in tops
                ]
                shifts = [top[0:1, :] for top in tops]

                def weigh(kv_ref, t, sums):
                    place = (kv_ref, 2 * t)
                    query_key(place, 0, base)
                    return weigh_values(place, 0, sums, shifts)

                sums = zero_sums
                for ref in kv_refs:
                    sums = lax.fori_loop(0, ref.shape[0] // 2, functools.partial(weigh, ref), sums)
                for m, at in enumerate(spans):
                    added = pltpu.matmul_pop(total[m])
                    max_ref[:, at] = tops[m]
                    if state_in is None:
                        acc_ref[:, at] = added
                        sum_ref[:, at] = sums[m]
                    else:
                        factor = jnp.exp2(old[m] - tops[m])
                        acc_ref[:, at] = state_in[0][:, at] * factor[0:1, :] + added
                        sum_ref[:, at] = state_in[1][:, at] * factor + sums[m]
                return carry

            lax.fori_loop(0, trips, trip, 0)

    specs = [pltpu.ACC(m)((rows, 256), jnp.float32) for _ in range(3) for m in range(2) for _ in range(4)]
    specs += [pltpu.ACC(m)((HD, 256), jnp.float32) for m in range(2)]
    pl.run_scoped(scoped, *specs)

    for step, final_ref in enumerate(final_refs):
        base = lax.rem(start + step, columns // 512) * 512
        for head in range(512 // HD):
            at = pl.ds(pl.multiple_of(base + head * HD, HD), HD)
            denom = jnp.sum(sum_ref[:, at], axis=0, keepdims=True)
            block = acc_ref[:, at] / denom
            final_ref[:, head * HD : (head + 1) * HD] = block.T.astype(jnp.bfloat16)


def attention_chunk(order, qt, kvs, query_gain, key_gain, state, steps):
    columns = qt.shape[1]
    first = state is None
    state_shapes = [
        jax.ShapeDtypeStruct((HD, columns), jnp.float32),
        jax.ShapeDtypeStruct((8, columns), jnp.float32),
        jax.ShapeDtypeStruct((8, columns), jnp.float32),
    ]
    keys = sum(kv.shape[0] for kv in kvs) * HD
    flops = 4 * columns * keys * HD // (2 if steps else 1)
    args = [order, qt, query_gain, key_gain, *kvs] + ([] if first else list(state))
    common = dict(
        in_specs=[pl.BlockSpec(memory_space=pl.ANY)] + [vspec()] * (len(args) - 1),
        compiler_params=pltpu.CompilerParams(vmem_limit_bytes=10 << 20),
        cost_estimate=pl.CostEstimate(flops=4 * flops, bytes_accessed=keys * 4 * HD, transcendentals=0),
        name="attention",
    )
    kernel = functools.partial(attention_kernel, first, steps, len(kvs))
    if steps:
        return pl.pallas_call(
            kernel,
            out_shape=[jax.ShapeDtypeStruct((HD, 512), jnp.bfloat16)] * len(steps),
            out_specs=[vspec()] * len(steps),
            scratch_shapes=[VM(s.shape, s.dtype) for s in state_shapes],
            **common,
        )(*args)
    return pl.pallas_call(
        kernel, out_shape=state_shapes, out_specs=[vspec()] * 3, **common
    )(*args)


def route_kernel(routes_ref, weight_ref, place_ref, mix_ref):
    rows, top = routes_ref.shape
    experts = place_ref.shape[0] // CAP
    slots = place_ref.shape[0]
    routes = routes_ref[...]
    weight = weight_ref[...]
    expert = lax.broadcasted_iota(jnp.int32, (rows, experts), 1)
    chosen = jnp.zeros((rows, experts), jnp.float32)
    amount = jnp.zeros((rows, experts), jnp.float32)
    for k in range(top):
        hit = routes[:, k : k + 1] == expert
        chosen = jnp.where(hit, 1.0, chosen)
        amount = jnp.where(hit, weight[:, k : k + 1], amount)
    earlier = (
        lax.broadcasted_iota(jnp.int32, (rows, rows), 0)
        > lax.broadcasted_iota(jnp.int32, (rows, rows), 1)
    ).astype(jnp.bfloat16)
    rank = jnp.dot(earlier, chosen.astype(jnp.bfloat16), preferred_element_type=jnp.float32)
    wide = (
        lax.broadcasted_iota(jnp.int32, (experts, slots), 1) // CAP
        == lax.broadcasted_iota(jnp.int32, (experts, slots), 0)
    ).astype(jnp.bfloat16)
    slot = (lax.broadcasted_iota(jnp.int32, (rows, slots), 1) % CAP).astype(jnp.float32)

    def spread(x):
        return jnp.dot(x.astype(jnp.bfloat16), wide, preferred_element_type=jnp.float32)

    mine = (spread(rank) == slot) & (spread(chosen) > 0.5)
    place_ref[...] = mine.astype(jnp.float32).T.astype(jnp.bfloat16)
    high = amount.astype(jnp.bfloat16).astype(jnp.float32)
    mix_ref[0:rows, :] = jnp.where(mine, spread(high), 0.0).astype(jnp.bfloat16)
    mix_ref[rows:, :] = jnp.where(mine, spread(amount - high), 0.0).astype(jnp.bfloat16)


def project_kernel(parts, *refs):
    head_refs = refs[:parts]
    weight_ref, residual_ref, gain_ref, place_ref, hidden_ref, normed_ref, send_ref = refs[parts:]
    depth = head_refs[0].shape[1]
    me = lax.axis_index("tp")
    total = residual_ref[...].astype(jnp.float32)
    for step, head_ref in enumerate(head_refs):
        part = lax.rem(me + parts - step, parts)
        weight = weight_ref[pl.ds(pl.multiple_of(part * depth, depth), depth), :]
        total = total + jnp.dot(head_ref[...], weight, preferred_element_type=jnp.float32)
    hidden = total.astype(jnp.bfloat16)
    hidden_ref[...] = hidden
    hidden = hidden.astype(jnp.float32)
    normed_ref[...] = (
        hidden
        * lax.rsqrt(jnp.mean(hidden * hidden, axis=-1, keepdims=True) + EPS)
        * gain_ref[...]
    ).astype(jnp.bfloat16)
    step = 256

    def place(i, carry):
        at = pl.ds(pl.multiple_of(i * step, step), step)
        send_ref[at, :] = jnp.dot(
            place_ref[at, :], normed_ref[...], preferred_element_type=jnp.float32
        ).astype(jnp.bfloat16)
        return carry

    lax.fori_loop(0, send_ref.shape[0] // step, place, 0)


def expert_kernel(arrived_ref, gate_ref, up_ref, down_ref, out_ref):
    step = 1024

    def block(i, carry):
        at = pl.ds(pl.multiple_of(i * step, step), step)
        x = arrived_ref[at, :]
        gate = jnp.dot(x, gate_ref[...], preferred_element_type=jnp.float32)
        up = jnp.dot(x, up_ref[...], preferred_element_type=jnp.float32)
        hidden = (jax.nn.silu(gate) * up).astype(jnp.bfloat16)
        out_ref[at, :] = jnp.dot(
            hidden, down_ref[...], preferred_element_type=jnp.float32
        ).astype(jnp.bfloat16)
        return carry

    lax.fori_loop(0, arrived_ref.shape[0] // step, block, 0)


def join_kernel(order_ref, *refs):
    out_ref = refs[-1]
    size = refs[0].shape[0]
    for i, ref in enumerate(refs[:-1]):
        out_ref[size * i : size * (i + 1)] = ref[...]


def combine_kernel(returned_ref, mix_ref, hidden_ref, normed_ref, sg_ref, su_ref, sd_ref, out_ref):
    normed = normed_ref[...]
    gate = jnp.dot(normed, sg_ref[...], preferred_element_type=jnp.float32)
    up = jnp.dot(normed, su_ref[...], preferred_element_type=jnp.float32)
    shared = (jax.nn.silu(gate) * up).astype(jnp.bfloat16)
    returned = returned_ref[...]
    total = jnp.dot(shared, sd_ref[...], preferred_element_type=jnp.float32)
    routed = jnp.dot(mix_ref[...], returned, preferred_element_type=jnp.float32)
    rows = total.shape[0]
    total = total + (routed[0:rows] + routed[rows:])
    out_ref[...] = (hidden_ref[...].astype(jnp.float32) + total).astype(jnp.bfloat16)


SIDE = 4


def shifted(x, stage, step):
    pairs = []
    for z in range(SIDE):
        for y in range(SIDE):
            for core in range(2):
                move_z = (core + stage) % 2 == 0
                to_z = (z + step) % SIDE if move_z else z
                to_y = y if move_z else (y + step) % SIDE
                pairs.append(((z * SIDE + y) * 2 + core, (to_z * SIDE + to_y) * 2 + core))
    return lax.ppermute(x, "sp", pairs)


def after(x, state):
    total, sums, tops = state
    *x, tops = lax.optimization_barrier((*x, tops))
    return x, (total, sums, tops)


def swapped(x):
    return lax.ppermute(x, "sp", [(i, i ^ 1) for i in range(2 * SIDE * SIDE)])


def body(
    queries,
    keys,
    values,
    residual,
    out_proj,
    query_gain,
    key_gain,
    norm_gain,
    routes,
    route_weight,
    expert_gate,
    expert_up,
    expert_down,
    shared_gate,
    shared_up,
    shared_down,
):
    tokens = queries.shape[0]
    columns = queries.shape[1] // HD * tokens
    rows = residual.shape[0]
    model = residual.shape[1]
    experts = expert_gate.shape[0] * lax.axis_size("sp") * lax.axis_size("tp")
    slots = experts * CAP
    cosine, sine = (jnp.asarray(t) for t in rotary_tables())
    qg, kg = query_gain.reshape(1, HD), key_gain.reshape(1, HD)
    bf16 = jnp.bfloat16
    shape = jax.ShapeDtypeStruct
    own = pl.pallas_call(
        kv_prep_kernel,
        out_shape=shape((tokens // HD, 2 * HD, HD), bf16),
        in_specs=[vspec()] * 5,
        out_specs=vspec(),
        name="kv_prep",
    )(keys, values, kg, cosine, sine)
    pieces = [shifted(own, 0, step) for step in (1, 3, 2)]
    qt, q_done = pl.pallas_call(
        q_prep_kernel,
        out_shape=[shape((2 * HD, columns), bf16), shape((8, HD), jnp.float32)],
        in_specs=[vspec()] * 4,
        out_specs=[vspec()] * 2,
        cost_estimate=pl.CostEstimate(flops=6 << 30, bytes_accessed=1 << 20, transcendentals=0),
        compiler_params=pltpu.CompilerParams(vmem_limit_bytes=56 << 20),
        name="q_prep",
    )(queries, qg, cosine, sine)
    place, mix = pl.pallas_call(
        route_kernel,
        out_shape=[shape((slots, rows), bf16), shape((2 * rows, slots), bf16)],
        in_specs=[vspec()] * 2,
        out_specs=[vspec()] * 2,
        cost_estimate=pl.CostEstimate(flops=2 << 30, bytes_accessed=1 << 20, transcendentals=0),
        compiler_params=pltpu.CompilerParams(vmem_limit_bytes=8 << 20),
        name="route",
    )(routes, route_weight)

    def attend(kvs, state, steps=(), order=query_gain):
        return attention_chunk(order, qt, kvs, qg, kg, state, steps)

    def join(pieces):
        return pl.pallas_call(
            join_kernel,
            out_shape=shape((len(pieces) * own.shape[0],) + own.shape[1:], bf16),
            in_specs=[pl.BlockSpec(memory_space=pl.ANY)] + [vspec()] * len(pieces),
            out_specs=vspec(),
            compiler_params=pltpu.CompilerParams(vmem_limit_bytes=6 << 20),
            name="join",
        )(q_done, *pieces)

    first, second = join([own, pieces[0]]), join(pieces[1:])
    up1, down2 = shifted(first, 1, 1), shifted(second, 1, 3)
    up2, down1 = shifted(second, 1, 1), shifted(first, 1, 3)
    twins = [swapped(first), swapped(second)]
    state = attend([first, second], None)
    state = attend(twins, state)
    (up1, down2), state = after([up1, down2], state)
    far1, far2 = shifted(up1, 1, 1), shifted(down2, 1, 3)
    twins = [swapped(up1), swapped(down2)]
    state = attend([up1, down2], state, order=place)
    (up2, down1), state = after([up2, down1], state)
    more = [swapped(up2), swapped(down1)]
    state = attend([*twins, up2, down1], state)
    (far1, far2), state = after([far1, far2], state)
    last = [swapped(far1), swapped(far2)]
    state = attend([*more, far1, far2], state)
    parts = columns // 512

    def exchanged(piece, step):
        return lax.ppermute(piece, "tp", [(i, (i + step) % parts) for i in range(parts)])

    one, two = attend(last, state, (1, 2))
    two, one = exchanged(two, 2), exchanged(one, 1)
    three, none = attend(last, state, (3, 4))
    heads = [none, one, two, exchanged(three, 3)]
    hidden1, normed, send = pl.pallas_call(
        functools.partial(project_kernel, parts),
        out_shape=[shape((rows, model), bf16), shape((rows, model), bf16), shape((slots, model), bf16)],
        in_specs=[vspec()] * (parts + 4),
        out_specs=[vspec()] * 3,
        compiler_params=pltpu.CompilerParams(vmem_limit_bytes=16 << 20),
        name="project",
    )(*heads, out_proj, residual, norm_gain.reshape(1, model), place)
    arrived = lax.all_to_all(
        send.reshape(experts, CAP, model), ("sp", "tp"), split_axis=0, concat_axis=0, tiled=True
    ).reshape(slots, model)
    processed = pl.pallas_call(
        expert_kernel,
        out_shape=shape((slots, model), bf16),
        in_specs=[vspec()] * 4,
        out_specs=vspec(),
        compiler_params=pltpu.CompilerParams(vmem_limit_bytes=24 << 20),
        name="experts",
    )(arrived, expert_gate[0], expert_up[0], expert_down[0])
    returned = lax.all_to_all(
        processed.reshape(experts, CAP, model), ("sp", "tp"), split_axis=0, concat_axis=0, tiled=True
    ).reshape(slots, model)
    return pl.pallas_call(
        combine_kernel,
        out_shape=shape((rows, model), bf16),
        in_specs=[vspec()] * 7,
        out_specs=vspec(),
        compiler_params=pltpu.CompilerParams(vmem_limit_bytes=16 << 20),
        name="combine",
    )(returned, mix, hidden1, normed, shared_gate, shared_up, shared_down)


def solution(mesh):
    placed = (
        P("sp", "tp"),
        P("sp", "tp"),
        P("sp", "tp"),
        P(("sp", "tp"), None),
        P(),
        P(),
        P(),
        P(),
        P(("sp", "tp"), None),
        P(("sp", "tp"), None),
        P(("sp", "tp"), None, None),
        P(("sp", "tp"), None, None),
        P(("sp", "tp"), None, None),
        P(),
        P(),
        P(),
    )
    return jax.shard_map(
        body, mesh=mesh, in_specs=placed, out_specs=P(("sp", "tp"), None), check_vma=False
    )
```
